32 devices in a mesh: fs: 16 (over z, y, x), tp: 2 (over core).
Axes of the slice: x: 2, y: 2, z: 4, core: 2. Of those that a mesh axis runs over, the one named last changes fastest.
Arguments:
- gate_pre: bfloat16 [8192, 3072], P('fs', 'tp'), may hold values from -6 to 6
- up_pre: bfloat16 [8192, 3072], P('fs', 'tp'), may hold values from -6 to 6
- cotangent: bfloat16 [8192, 2048], P('fs'), may hold values from -8 to 8
- gate_weight: bfloat16 [2048, 3072], P('fs', 'tp'), may hold values from -0.125 to 0.125
- up_weight: bfloat16 [2048, 3072], P('fs', 'tp'), may hold values from -0.125 to 0.125
- down_weight: bfloat16 [2048, 3072], P('fs', 'tp'), may hold values from -0.109375 to 0.109375
Outputs:
- grad_input: bfloat16 [8192, 2048], P('fs')
- grad_down: float32 [2048, 3072], P('fs', 'tp')
The draws below stay inside these ranges and needn't reach their ends.
All inputs are finite; a program needn't handle non-finite values.
Results may differ from the reference program's by a relative error of at most 0.014.
Values may be sent and summed in bfloat16 or wider, within the bound.
A program may use at most 128 MiB of HBM per device.

```python
import jax
import jax.numpy as jnp
from jax import lax

D = 2048
FF = 3072
TOKENS = 8192
N_TP = 2


def strengthened(result, stream_key, source, target, blocks, factor):
    def block_of(position):
        return (jnp.arange(result.shape[position]) // (result.shape[position] // blocks)).reshape((-1,) + (1,) * (result.ndim - 1 - position))

    one_side = jax.random.permutation(stream_key, blocks)[block_of(target)]
    far = (block_of(target) + blocks // 2) % blocks
    return jnp.where((block_of(source) == one_side) | (block_of(source) == far), factor * result, result)


def steps_of(stream_key, shape, pieces, smallest, top_value):
    factor_of, own = 1.0, jax.random.fold_in(stream_key, 6)
    for position, shards_of in pieces:
        heights = jnp.exp(jax.random.uniform(jax.random.fold_in(own, position), (shards_of,), jnp.float32, smallest / len(pieces), top_value / len(pieces)))
        factor_of = factor_of * jnp.repeat(heights, shape[position] // shards_of).reshape([-1 if axis == position else 1 for axis in range(len(shape))])
    return factor_of


def noise(rng, extent, scale, most, split=(), held_as=jnp.bfloat16):
    drawn = scale * jax.random.normal(rng, extent, jnp.float32)
    if split:
        drawn = drawn * steps_of(rng, extent, split, -0.22, 0.18)
    return jnp.clip(drawn, -most, most).astype(held_as)


def gaussian_with(rng, shape, scale, bound, pieces, heavy, dtype=jnp.bfloat16):
    drawn = scale * jax.random.normal(rng, shape, jnp.float32)
    if pieces:
        drawn = drawn * steps_of(rng, shape, pieces, -0.22, 0.18)
    return jnp.clip(strengthened(drawn, jax.random.fold_in(rng, 3), *heavy), -bound, bound).astype(dtype)


def setup_inputs(seed: int = 0) -> dict:
    arg_keys = jax.random.split(jax.random.key(seed), 7)
    gate_pre = noise(arg_keys[0], (TOKENS, FF), 1.0, 6.0, ((0, 16), (1, 2)))
    up_pre = noise(arg_keys[1], (TOKENS, FF), 1.0, 6.0, ((0, 16), (1, 2)))
    cotangent = gaussian_with(arg_keys[2], (TOKENS, D), 1.0, 8.0, ((0, 16),), (0, 1, 16, 2.0))
    gate_weight = noise(arg_keys[3], (D, FF), D ** -0.5, 0.125, ((0, 16), (1, 2)))
    up_weight = noise(arg_keys[4], (D, FF), D ** -0.5, 0.125, ((0, 16), (1, 2)))
    down_weight = noise(arg_keys[5], (D, FF), FF ** -0.5, 0.109375, ((0, 16), (1, 2)))
    return dict(gate_pre=gate_pre, up_pre=up_pre, cotangent=cotangent, gate_weight=gate_weight, up_weight=up_weight, down_weight=down_weight)


def reference(gate_pre, up_pre, cotangent, gate_weight, up_weight, down_weight):
    gate = gate_pre.astype(jnp.float32)
    upper = up_pre.astype(jnp.float32)
    sigma = jax.nn.sigmoid(gate)
    hidden = (gate * sigma * upper).astype(jnp.bfloat16)
    d_hidden = jnp.dot(cotangent, down_weight, preferred_element_type=jnp.float32)
    d_gate = (d_hidden * upper * sigma * (1.0 + gate * (1.0 - sigma))).astype(jnp.bfloat16)
    d_up = (d_hidden * gate * sigma).astype(jnp.bfloat16)
    grad_down = lax.dot_general(cotangent, hidden, (((0,), (0,)), ((), ())), preferred_element_type=jnp.float32)
    width = FF // N_TP
    total = jnp.zeros((cotangent.shape[0], D), jnp.float32)
    for block in range(N_TP):
        lower = block * width
        part = lax.dot_general(d_gate[:, lower:lower + width], gate_weight[:, lower:lower + width], (((1,), (1,)), ((), ())), preferred_element_type=jnp.float32)
        part = part + lax.dot_general(d_up[:, lower:lower + width], up_weight[:, lower:lower + width], (((1,), (1,)), ((), ())), preferred_element_type=jnp.float32)
        total = total + part.astype(jnp.bfloat16).astype(jnp.float32)
    return total.astype(jnp.bfloat16), grad_down
```

```python
import functools

import jax
import jax.numpy as jnp
from jax import lax
from jax.experimental import pallas as pl
from jax.experimental.pallas import tpu as pltpu
from jax.sharding import PartitionSpec as P

MESH = pl.DeviceIdType.MESH
F32, BF16 = jnp.float32, jnp.bfloat16
LANES = 128
VMEM_LIMIT = 62 * 1024 * 1024
GROUP, OUTER, PARTS = 4, 4, 2
OVER = (((1,), (1,)), ((), ()))
DOWN = (((0,), (0,)), ((), ()))


def at(index, size):
    return pl.ds(pl.multiple_of(index * size, size), size)


def remote(src, dst, send, recv, device):
    return pltpu.make_async_remote_copy(
        src_ref=src, dst_ref=dst, send_sem=send, recv_sem=recv, device_id=device, device_id_type=MESH
    )


def greet(devices):
    barrier = pltpu.get_barrier_semaphore()
    for device in devices:
        pl.semaphore_signal(barrier, inc=1, device_id=device, device_id_type=MESH)
    pl.semaphore_wait(barrier, len(devices))


def layer_kernel(
    cot, gate, up, gate_w, up_w, down_w, out, gd,
    cots, downs, pair_w, gates, ups, dh, hidden, dpair, acc, share,
    give, sib, mine, got, halves, comb, joined, reduced, final, swapped,
    send, recv, zsend, zrecv, rsend, rrecv, own,
):
    g = GROUP
    fs, core = lax.axis_index("fs"), lax.axis_index("tp")
    outer, me = lax.div(fs, g), lax.rem(fs, g)
    base = outer * g
    x, y = lax.rem(me, 2), lax.div(me, 2)
    xn, yn, far = y * 2 + (1 - x), (1 - y) * 2 + x, 3 - me
    xdev, ydev, fdev, sibling = (base + xn, core), (base + yn, core), (base + far, core), (fs, 1 - core)
    others = [(far, fdev), (xn, xdev), (yn, ydev)]
    level = lambda o: (o * g + me, core)
    tokens, depth = cot.shape
    rows, part = down_w.shape[0], downs.shape[1]
    block = rows * g
    half, wide = tokens // 2, depth // 2
    edge = (outer == 0) | (outer == OUTER - 1)
    middle = jnp.logical_not(edge)
    low = outer < OUTER // 2

    greet([d for _, d in others] + [sibling] + [level(lax.rem(outer + k, OUTER)) for k in range(1, OUTER)])

    started, count = [], [0]

    def go(src, dst, device):
        n = count[0]
        count[0] += 1
        c = remote(src, dst, send.at[n], recv.at[n], device)
        c.start()
        started.append(c)
        return c

    local = []

    def keep_local(src, dst):
        c = pltpu.make_async_copy(src, dst, own.at[len(local)])
        c.start()
        local.append(c)
        return c

    place = at(fs, rows)
    sides = [pl.ds(0, part), pl.ds(part, part)]
    swap_down = [go(down_w.at[:, at(q, part)], downs.at[place, :], d) for q, d in others]
    own_down = keep_local(down_w.at[:, at(me, part)], downs.at[place, :])
    swap_pair = []
    own_pair = []
    for w, side in ((gate_w, sides[0]), (up_w, sides[1])):
        swap_pair += [go(w.at[:, at(q, part)], pair_w.at[place, side], d) for q, d in others]
        own_pair.append(keep_local(w.at[:, at(me, part)], pair_w.at[place, side]))

    cols = [pl.ds(0, wide), pl.ds(wide, wide)]
    piece = lambda owner, i: cots.at[at(owner * 2 + core, half), cols[i]]
    row_half = at(core, half)
    x0 = go(cot.at[row_half, cols[0]], piece(me, 0), xdev)
    y1 = go(cot.at[row_half, cols[1]], piece(me, 1), ydev)
    x1 = go(cot.at[row_half, cols[1]], piece(me, 1), xdev)
    y0 = go(cot.at[row_half, cols[0]], piece(me, 0), ydev)
    own_cot = keep_local(cot, cots.at[at(me, tokens), :])
    mine_of = at(me, tokens)
    own_gate = keep_local(gate.at[:, at(me, part)], gates.at[mine_of, :])
    own_up = keep_local(up.at[:, at(me, part)], ups.at[mine_of, :])

    def pass_on(owner, i):
        return go(piece(owner, i), piece(owner, i), sibling)

    def zblock(j, b):
        if j == 0:
            return downs.at[at(b, block), :]
        return pair_w.at[at(b * 2 + (j - 1), block // 2), :]

    def nearest(k):
        a = jnp.where(edge, k, (1, 2, 0, 3)[k])
        return jnp.where(low, a, OUTER - 1 - a)

    above, below = level(jnp.minimum(outer + 1, OUTER - 1)), level(jnp.maximum(outer - 1, 0))

    def zown(j):
        b = zblock(j, outer)
        return [
            (outer < OUTER - 1, remote(b, b, zsend.at[j, 0], zrecv.at[j, outer], above)),
            (outer > 0, remote(b, b, zsend.at[j, 1], zrecv.at[j, outer], below)),
        ]

    line_sends = []

    def zstart(j, only):
        for cond, c in zown(j):

            @pl.when(cond & only)
            def _():
                c.start()

    def zcopy(j, k):
        b = nearest(k)
        target = level(jnp.clip(jnp.where(b > outer, outer - 1, outer + 1), 0, OUTER - 1))
        return remote(zblock(j, b), zblock(j, b), zsend.at[j, 1 + k], zrecv.at[j, b], target)

    def zforward(j, k):
        c = zcopy(j, k)

        @pl.when(middle)
        def _():
            c.wait_recv()
            c.start()

    def zarrive(j, k):
        c = zcopy(j, k)

        @pl.when(edge)
        def _():
            c.wait_recv()

    tile = tokens // 2

    def d_hidden(owner):
        def step(i, carry):
            r = at(owner * 2 + i, tile)
            dh[r, :] = jnp.dot(cots[r, :], downs[...], preferred_element_type=F32)
            return carry

        lax.fori_loop(0, 2, step, 0)

    strip = tokens // 16

    def pointwise(owner):
        def step(i, carry):
            r = at(owner * 16 + i, strip)
            gv, uv, dv = gates[r, :].astype(F32), ups[r, :].astype(F32), dh[r, :]
            s = jax.nn.sigmoid(gv)
            gs = gv * s
            hidden[r, :] = (gs * uv).astype(BF16)
            dpair[r, sides[0]] = (dv * uv * s * (1.0 + gv * (1.0 - s))).astype(BF16)
            dpair[r, sides[1]] = (dv * gs).astype(BF16)
            return carry

        lax.fori_loop(0, 16, step, 0)

    span = depth // 8

    def outer_product(owner, first=False, last=False):
        r = at(owner, tokens)

        def step(i, carry):
            d = at(i, span)
            new = lax.dot_general(cots[r, d], hidden[r, :], DOWN, preferred_element_type=F32)
            if not first:
                new = new + acc[d, :]
            acc[d, :] = new
            if last:
                share[d, :] = new.astype(BF16)
            return carry

        lax.fori_loop(0, 8, step, 0)

    lane = block // 2

    def product(p, owner, side, dst):
        r = at(owner, tokens)

        def step(i, carry):
            b = jnp.where(i == 0, nearest(2 * p), nearest(2 * p + 1))
            total = lax.dot_general(
                dpair[r, :], pair_w[at(b * 2 + side, lane), :], OVER, preferred_element_type=F32
            )
            dst[:, at(i, lane)] = total.astype(BF16)
            return carry

        lax.fori_loop(0, 2, step, 0)

    def add(dst, where, src):
        dst[where, :] = (dst[where, :].astype(F32) + src[...].astype(F32)).astype(BF16)

    slot = {}

    def give_away(p, n, owner):
        k = p * 4 + n
        product(p, owner, 1 - core, give.at[k])
        slot[k] = go(give.at[k], sib.at[k], sibling)

    def keep_own(p, n, owner):
        product(p, owner, core, mine.at[p * 4 + n])

    def join(p, n):
        k = p * 4 + n
        slot[k].wait_recv()
        add(mine.at[k], pl.ds(0, tokens), sib.at[k])

    top, bottom = pl.ds(0, half), pl.ds(half, half)
    crossing, arrivals = {}, {}

    def send_far(p):
        k = p * 4
        crossing[p, 0] = go(mine.at[k, top, :], halves.at[p, 0], xdev)
        crossing[p, 1] = go(mine.at[k, bottom, :], halves.at[p, 1], ydev)

    def send_x(p):
        arrivals[p, 0] = go(mine.at[p * 4 + 1, top, :], got.at[p, 0, top, :], xdev)

    def send_y(p):
        arrivals[p, 1] = go(mine.at[p * 4 + 2, bottom, :], got.at[p, 1, bottom, :], ydev)

    def relay(p):
        crossing[p, 1].wait_recv()
        add(mine.at[p * 4 + 1], bottom, halves.at[p, 1])
        arrivals[p, 2] = go(mine.at[p * 4 + 1, bottom, :], got.at[p, 0, bottom, :], xdev)
        crossing[p, 0].wait_recv()
        add(mine.at[p * 4 + 2], top, halves.at[p, 0])
        arrivals[p, 3] = go(mine.at[p * 4 + 2, top, :], got.at[p, 1, top, :], ydev)

    lasts = []

    def finish(p):
        for i in range(4):
            arrivals[p, i].wait_recv()
        for i in range(2):
            c = pl.ds(i * lane, lane)
            total = mine[p * 4 + 3, :, c].astype(F32) + got[p, 0, :, c].astype(F32) + got[p, 1, :, c].astype(F32)
            where = at(nearest(2 * p + i) * 2 + core, lane)
            out[:, where] = total.astype(BF16)
            lasts.append(go(out.at[:, where], out.at[:, where], sibling))

    near = jnp.where(low, 1 - outer, 5 - outer)
    cross_mid = jnp.where(low, 2, 1)
    cross_edge = jnp.where(low, 3, 0)
    edge_sends = [
        remote(share.at[at(cross_edge, block), :], comb.at[1], rsend.at[0], rrecv.at[0], level(near)),
        remote(share.at[at(cross_mid, block), :], comb.at[0], rsend.at[1], rrecv.at[1], level(near)),
    ]
    near_send = remote(share.at[at(near, block), :], reduced.at[0], rsend.at[2], rrecv.at[2], level(near))
    cross_sends = [
        remote(joined.at[1], reduced.at[1], rsend.at[0], rrecv.at[3], level(cross_edge)),
        remote(joined.at[0], reduced.at[1], rsend.at[1], rrecv.at[3], level(cross_mid)),
    ]

    def reduce_start():
        @pl.when(edge)
        def _():
            for c in edge_sends:
                c.start()

        near_send.start()

    def reduce_join():
        @pl.when(middle)
        def _():
            for i, dest in ((1, cross_edge), (0, cross_mid)):
                edge_sends[1 - i].wait_recv()
                joined[i] = (share[at(dest, block), :].astype(F32) + comb[i].astype(F32)).astype(BF16)
                cross_sends[1 - i].start()

    gd_sends = []

    def reduce_finish():
        near_send.wait_recv()
        cross_sends[0].wait_recv()
        total = acc[at(outer, block), :] + reduced[0].astype(F32) + reduced[1].astype(F32)
        final[...] = total.astype(BF16)
        for i, (q, d) in enumerate(others):
            gd_sends.append(go(final.at[at(q, rows), :], swapped.at[i], d))
        gd[:, at(me, part)] = final[at(me, rows), :].astype(F32)

    yes = outer >= 0
    own_down.wait()
    for c in swap_down:
        c.wait_recv()
    zstart(0, yes)
    for c in own_pair:
        c.wait()
    for c in swap_pair:
        c.wait_recv()
    for k in (1, 2):
        zforward(0, k)
        zarrive(0, k)
    for j in (1, 2):
        zstart(j, edge)
    zforward(0, 3)
    zarrive(0, 3)
    for j in (1, 2):
        zstart(j, middle)
    passes = {}
    x0.wait_recv()
    fy = go(piece(xn, 0), piece(xn, 0), ydev)
    passes["x", 0] = pass_on(xn, 0)
    y1.wait_recv()
    fx = go(piece(yn, 1), piece(yn, 1), xdev)
    passes["y", 1] = pass_on(yn, 1)
    arrive = {}
    for name, (q, d) in zip("fxy", others):
        arrive[name] = [
            go(a.at[:, at(q, part)], b.at[mine_of, :], d) for a, b in ((gate, gates), (up, ups))
        ]
    own_cot.wait()
    own_gate.wait()
    own_up.wait()
    d_hidden(me)
    pointwise(me)
    outer_product(me, first=True)
    x1.wait_recv()
    passes["x", 1] = pass_on(xn, 1)
    y0.wait_recv()
    passes["y", 0] = pass_on(yn, 0)
    for j in (1, 2):
        for k in (1, 2):
            zforward(j, k)
    fy.wait_recv()
    passes["f", 0] = pass_on(far, 0)
    fx.wait_recv()
    passes["f", 1] = pass_on(far, 1)
    zforward(1, 3)
    for name, owner in (("x", xn), ("y", yn), ("f", far)):
        for i in range(2):
            passes[name, i].wait_recv()
        d_hidden(owner)
        if name == "y":
            zforward(2, 3)

    for c in arrive["f"]:
        c.wait_recv()
    pointwise(far)
    for j in (1, 2):
        zarrive(j, 1)
    give_away(0, 0, far)
    keep_own(0, 0, far)
    give_away(0, 3, me)
    join(0, 0)
    send_far(0)
    keep_own(0, 3, me)
    outer_product(far)
    join(0, 3)
    for c in arrive["x"]:
        c.wait_recv()
    pointwise(xn)
    give_away(0, 1, xn)
    keep_own(0, 1, xn)
    for c in arrive["y"]:
        c.wait_recv()
    pointwise(yn)
    join(0, 1)
    send_x(0)
    give_away(0, 2, yn)
    keep_own(0, 2, yn)
    outer_product(xn)
    join(0, 2)
    send_y(0)
    outer_product(yn, last=True)
    reduce_start()
    relay(0)
    for k in (2, 3):
        for j in (1, 2):
            zarrive(j, k)
    give_away(1, 0, far)
    keep_own(1, 0, far)
    give_away(1, 1, xn)
    join(1, 0)
    send_far(1)
    keep_own(1, 1, xn)
    give_away(1, 2, yn)
    join(1, 1)
    send_x(1)
    keep_own(1, 2, yn)
    give_away(1, 3, me)
    join(1, 2)
    send_y(1)
    keep_own(1, 3, me)
    reduce_join()
    join(1, 3)
    finish(0)
    relay(1)
    reduce_finish()
    finish(1)
    for i, (q, _) in enumerate(others):
        gd_sends[i].wait_recv()
        gd[:, at(q, part)] = swapped[i].astype(F32)
    for c in lasts:
        c.wait_recv()
    for c in started:
        c.wait_send()
    for j in range(3):
        for cond, c in zown(j):

            @pl.when(cond)
            def _():
                c.wait_send()

    @pl.when(middle)
    def _():
        for j in range(3):
            for k in (1, 2, 3):
                zcopy(j, k).wait_send()
        for c in cross_sends:
            c.wait_send()

    @pl.when(edge)
    def _():
        for c in edge_sends:
            c.wait_send()

    near_send.wait_send()


def layer(gate_pre, up_pre, cotangent, gate_weight, up_weight, down_weight):
    tokens, width = gate_pre.shape
    rows, depth = gate_weight.shape[0], cotangent.shape[1]
    g = GROUP
    part, block, everyone = width // g, rows * g, tokens * g
    lane, half = block // 2, tokens // 2
    sems, vmem = pltpu.SemaphoreType.DMA, pltpu.VMEM
    struct = jax.ShapeDtypeStruct
    hbm = pl.BlockSpec(memory_space=pl.ANY)
    whole = pl.BlockSpec(memory_space=pltpu.VMEM)
    n = 72
    return pl.pallas_call(
        layer_kernel,
        out_shape=[struct((tokens, depth), BF16), struct((rows, width), F32)],
        in_specs=[hbm] * 6,
        out_specs=[whole] * 2,
        scratch_shapes=[
            vmem((everyone, depth), BF16),
            vmem((depth, part), BF16),
            vmem((depth, 2 * part), BF16),
            vmem((everyone, part), BF16),
            vmem((everyone, part), BF16),
            vmem((everyone, part), F32),
            vmem((everyone, part), BF16),
            vmem((everyone, 2 * part), BF16),
            vmem((depth, part), F32),
            vmem((depth, part), BF16),
            vmem((PARTS * 4, tokens, 2 * lane), BF16),
            vmem((PARTS * 4, tokens, 2 * lane), BF16),
            vmem((PARTS * 4, tokens, 2 * lane), BF16),
            vmem((PARTS, 2, tokens, 2 * lane), BF16),
            vmem((PARTS, 2, half, 2 * lane), BF16),
            vmem((2, block, part), BF16),
            vmem((2, block, part), BF16),
            vmem((2, block, part), BF16),
            vmem((block, part), BF16),
            vmem((3, rows, part), BF16),
            sems((n,)), sems((n,)), sems((3, 5)), sems((3, OUTER)), sems((3,)), sems((4,)), sems((6,)),
        ],
        compiler_params=pltpu.CompilerParams(
            collective_id=0, has_side_effects=True, vmem_limit_bytes=VMEM_LIMIT
        ),
    )(cotangent, gate_pre, up_pre, gate_weight, up_weight, down_weight)


def plain(gate_pre, up_pre, cotangent, gate_weight, up_weight, down_weight):
    gate = gate_pre.astype(F32)
    upper = up_pre.astype(F32)
    sigma = jax.nn.sigmoid(gate)
    hidden = (gate * sigma * upper).astype(BF16)
    share = lax.dot_general(cotangent, hidden, DOWN, preferred_element_type=F32)
    grad_down = lax.psum_scatter(share, "fs", scatter_dimension=0, tiled=True)
    d_hidden = jnp.dot(cotangent, lax.all_gather(down_weight, "fs", axis=0, tiled=True), preferred_element_type=F32)
    d_gate = (d_hidden * upper * sigma * (1.0 + gate * (1.0 - sigma))).astype(BF16)
    d_up = (d_hidden * gate * sigma).astype(BF16)
    gate_w, up_w = lax.all_gather((gate_weight, up_weight), "fs", axis=0, tiled=True)
    partial_sum = lax.dot_general(d_gate, gate_w, OVER, preferred_element_type=F32)
    partial_sum = partial_sum + lax.dot_general(d_up, up_w, OVER, preferred_element_type=F32)
    grad_input = lax.psum(partial_sum.astype(BF16), "tp").astype(F32).astype(BF16)
    return grad_input, grad_down


def solution(mesh):
    n_fs, n_tp = mesh.shape["fs"], mesh.shape["tp"]

    def local(*args):
        tokens, width = args[0].shape
        rows, depth = args[3].shape[0], args[2].shape[1]
        fits = n_tp == 2 and n_fs == GROUP * OUTER and width % (GROUP * LANES) == 0
        fits = fits and rows % 64 == 0 and tokens % 512 == 0 and depth == rows * n_fs
        return layer(*args) if fits else plain(*args)

    both, rows = P("fs", "tp"), P("fs", None)
    return jax.shard_map(
        local, mesh=mesh, in_specs=(both, both, rows, both, both, both), out_specs=(rows, both), check_vma=False
    )
```

```python
import functools

import jax
import jax.numpy as jnp
from jax import lax
from jax.experimental import pallas as pl
from jax.experimental.pallas import tpu as pltpu
from jax.sharding import PartitionSpec as P

MESH = pl.DeviceIdType.MESH
F32, BF16 = jnp.float32, jnp.bfloat16
LANES = 128
VMEM_LIMIT = 58 * 1024 * 1024
GROUP, OUTER, PARTS = 4, 4, 2
OVER = (((1,), (1,)), ((), ()))
DOWN = (((0,), (0,)), ((), ()))


def at(index, size):
    return pl.ds(pl.multiple_of(index * size, size), size)


def remote(src, dst, send, recv, device):
    return pltpu.make_async_remote_copy(
        src_ref=src, dst_ref=dst, send_sem=send, recv_sem=recv, device_id=device, device_id_type=MESH
    )


def greet(devices):
    barrier = pltpu.get_barrier_semaphore()
    for device in devices:
        pl.semaphore_signal(barrier, inc=1, device_id=device, device_id_type=MESH)
    pl.semaphore_wait(barrier, len(devices))


def layer_kernel(
    cot, gate, up, gate_w, up_w, down_w, out, gd,
    cots, downs, pair_w, gates, ups, dh, hidden, dpair, acc, share,
    give, sib, mine, got, halves, comb, joined, reduced, final, swapped,
    send, recv, zsend, zrecv, rsend, rrecv, own,
):
    g = GROUP
    fs, core = lax.axis_index("fs"), lax.axis_index("tp")
    outer, me = lax.div(fs, g), lax.rem(fs, g)
    base = outer * g
    x, y = lax.rem(me, 2), lax.div(me, 2)
    xn, yn, far = y * 2 + (1 - x), (1 - y) * 2 + x, 3 - me
    xdev, ydev, fdev, sibling = (base + xn, core), (base + yn, core), (base + far, core), (fs, 1 - core)
    others = [(far, fdev), (xn, xdev), (yn, ydev)]
    level = lambda o: (o * g + me, core)
    tokens, depth = cot.shape
    rows, part = down_w.shape[0], downs.shape[1]
    block = rows * g
    half, wide = tokens // 2, depth // 2
    edge = (outer == 0) | (outer == OUTER - 1)
    middle = jnp.logical_not(edge)
    low = outer < OUTER // 2

    greet([d for _, d in others] + [sibling] + [level(lax.rem(outer + k, OUTER)) for k in range(1, OUTER)])

    started, count = [], [0]

    def go(src, dst, device):
        n = count[0]
        count[0] += 1
        c = remote(src, dst, send.at[n], recv.at[n], device)
        c.start()
        started.append(c)
        return c

    local = []

    def keep_local(src, dst):
        c = pltpu.make_async_copy(src, dst, own.at[len(local)])
        c.start()
        local.append(c)
        return c

    place = at(fs, rows)
    sides = [pl.ds(0, part), pl.ds(part, part)]
    swap_down = [go(down_w.at[:, at(q, part)], downs.at[place, :], d) for q, d in others]
    own_down = keep_local(down_w.at[:, at(me, part)], downs.at[place, :])
    swap_pair = []
    own_pair = []
    for w, side in ((gate_w, sides[0]), (up_w, sides[1])):
        swap_pair += [go(w.at[:, at(q, part)], pair_w.at[place, side], d) for q, d in others]
        own_pair.append(keep_local(w.at[:, at(me, part)], pair_w.at[place, side]))

    cols = [pl.ds(0, wide), pl.ds(wide, wide)]
    piece = lambda owner, i: cots.at[at(owner * 2 + core, half), cols[i]]
    row_half = at(core, half)
    x0 = go(cot.at[row_half, cols[0]], piece(me, 0), xdev)
    y1 = go(cot.at[row_half, cols[1]], piece(me, 1), ydev)
    x1 = go(cot.at[row_half, cols[1]], piece(me, 1), xdev)
    y0 = go(cot.at[row_half, cols[0]], piece(me, 0), ydev)
    own_cot = keep_local(cot, cots.at[at(me, tokens), :])
    mine_of = at(me, tokens)
    own_gate = keep_local(gate.at[:, at(me, part)], gates.at[mine_of, :])
    own_up = keep_local(up.at[:, at(me, part)], ups.at[mine_of, :])

    def pass_on(owner, i):
        return go(piece(owner, i), piece(owner, i), sibling)

    def zblock(j, b):
        if j == 0:
            return downs.at[at(b, block), :]
        return pair_w.at[at(b * 2 + (j - 1), block // 2), :]

    def nearest(k):
        a = jnp.where(edge, k, (1, 2, 0, 3)[k])
        return jnp.where(low, a, OUTER - 1 - a)

    above, below = level(jnp.minimum(outer + 1, OUTER - 1)), level(jnp.maximum(outer - 1, 0))

    def zown(j):
        b = zblock(j, outer)
        return [
            (outer < OUTER - 1, remote(b, b, zsend.at[j, 0], zrecv.at[j, outer], above)),
            (outer > 0, remote(b, b, zsend.at[j, 1], zrecv.at[j, outer], below)),
        ]

    line_sends = []

    def zstart(j, only):
        for cond, c in zown(j):

            @pl.when(cond & only)
            def _():
                c.start()

    def zcopy(j, k):
        b = nearest(k)
        target = level(jnp.clip(jnp.where(b > outer, outer - 1, outer + 1), 0, OUTER - 1))
        return remote(zblock(j, b), zblock(j, b), zsend.at[j, 1 + k], zrecv.at[j, b], target)

    def zforward(j, k):
        c = zcopy(j, k)

        @pl.when(middle)
        def _():
            c.wait_recv()
            c.start()

    def zarrive(j, k):
        c = zcopy(j, k)

        @pl.when(edge)
        def _():
            c.wait_recv()

    tile = tokens // 2

    def d_hidden(owner):
        def step(i, carry):
            r = at(owner * 2 + i, tile)
            dh[r, :] = jnp.dot(cots[r, :], downs[...], preferred_element_type=F32)
            return carry

        lax.fori_loop(0, 2, step, 0)

    strip = tokens // 16
    first_cut = part // LANES * 2 // 3 * LANES
    cuts, everything = [(0, first_cut), (first_cut, part - first_cut)], (0, part)

    def pointwise(owner, cut):
        c, second = pl.ds(*cut), pl.ds(part + cut[0], cut[1])

        def step(i, carry):
            r = at(owner * 16 + i, strip)
            gv, uv, dv = gates[r, c].astype(F32), ups[r, c].astype(F32), dh[r, c]
            s = jax.nn.sigmoid(gv)
            gs = gv * s
            hidden[r, c] = (gs * uv).astype(BF16)
            dpair[r, c] = (dv * uv * s * (1.0 + gv * (1.0 - s))).astype(BF16)
            dpair[r, second] = (dv * gs).astype(BF16)
            return carry

        lax.fori_loop(0, 16, step, 0)

    span = depth // 8

    def outer_product(owner, cut, first=False, last=False):
        r, c = at(owner, tokens), pl.ds(*cut)

        def step(i, carry):
            d = at(i, span)
            new = lax.dot_general(cots[r, d], hidden[r, c], DOWN, preferred_element_type=F32)
            if not first:
                new = new + acc[d, c]
            acc[d, c] = new
            if last:
                share[d, c] = new.astype(BF16)
            return carry

        lax.fori_loop(0, 8, step, 0)

    lane = block // 2

    def product(p, owner, side, dst):
        r = at(owner, tokens)

        def step(i, carry):
            b = jnp.where(i == 0, nearest(2 * p), nearest(2 * p + 1))
            total = lax.dot_general(
                dpair[r, :], pair_w[at(b * 2 + side, lane), :], OVER, preferred_element_type=F32
            )
            dst[:, at(i, lane)] = total.astype(BF16)
            return carry

        lax.fori_loop(0, 2, step, 0)

    def add(dst, where, src):
        dst[where, :] = (dst[where, :].astype(F32) + src[...].astype(F32)).astype(BF16)

    slot = {}

    def give_away(p, n, owner):
        k = p * 4 + n
        product(p, owner, 1 - core, give.at[k])
        slot[k] = go(give.at[k], sib.at[k], sibling)

    def keep_own(p, n, owner):
        product(p, owner, core, mine.at[p * 4 + n])

    def join(p, n):
        k = p * 4 + n
        slot[k].wait_recv()
        add(mine.at[k], pl.ds(0, tokens), sib.at[k])

    top, bottom = pl.ds(0, half), pl.ds(half, half)
    crossing, arrivals = {}, {}

    def send_far(p):
        k = p * 4
        crossing[p, 0] = go(mine.at[k, top, :], halves.at[p, 0], xdev)
        crossing[p, 1] = go(mine.at[k, bottom, :], halves.at[p, 1], ydev)

    def send_x(p):
        arrivals[p, 0] = go(mine.at[p * 4 + 1, top, :], got.at[p, 0, top, :], xdev)

    def send_y(p):
        arrivals[p, 1] = go(mine.at[p * 4 + 2, bottom, :], got.at[p, 1, bottom, :], ydev)

    def relay(p):
        crossing[p, 1].wait_recv()
        add(mine.at[p * 4 + 1], bottom, halves.at[p, 1])
        arrivals[p, 2] = go(mine.at[p * 4 + 1, bottom, :], got.at[p, 0, bottom, :], xdev)
        crossing[p, 0].wait_recv()
        add(mine.at[p * 4 + 2], top, halves.at[p, 0])
        arrivals[p, 3] = go(mine.at[p * 4 + 2, top, :], got.at[p, 1, top, :], ydev)

    lasts = []

    def finish(p):
        for i in range(4):
            arrivals[p, i].wait_recv()
        for i in range(2):
            c = pl.ds(i * lane, lane)
            total = mine[p * 4 + 3, :, c].astype(F32) + got[p, 0, :, c].astype(F32) + got[p, 1, :, c].astype(F32)
            where = at(nearest(2 * p + i) * 2 + core, lane)
            out[:, where] = total.astype(BF16)
            lasts.append(go(out.at[:, where], out.at[:, where], sibling))

    near = jnp.where(low, 1 - outer, 5 - outer)
    cross_mid = jnp.where(low, 2, 1)
    cross_edge = jnp.where(low, 3, 0)
    edge_sends, near_sends, cross_sends = [], [], []
    for t, cut in enumerate(cuts):
        c = pl.ds(*cut)
        edge_sends.append([
            remote(share.at[at(cross_edge, block), c], comb.at[1, :, c], rsend.at[t, 0], rrecv.at[t, 0], level(near)),
            remote(share.at[at(cross_mid, block), c], comb.at[0, :, c], rsend.at[t, 1], rrecv.at[t, 1], level(near)),
        ])
        near_sends.append(
            remote(share.at[at(near, block), c], reduced.at[0, :, c], rsend.at[t, 2], rrecv.at[t, 2], level(near))
        )
        cross_sends.append([
            remote(joined.at[1, :, c], reduced.at[1, :, c], rsend.at[t, 0], rrecv.at[t, 3], level(cross_edge)),
            remote(joined.at[0, :, c], reduced.at[1, :, c], rsend.at[t, 1], rrecv.at[t, 3], level(cross_mid)),
        ])

    def reduce_start(t):
        @pl.when(edge)
        def _():
            for c in edge_sends[t]:
                c.start()

        near_sends[t].start()

    def reduce_join(t):
        c = pl.ds(*cuts[t])

        @pl.when(middle)
        def _():
            for i, dest in ((1, cross_edge), (0, cross_mid)):
                edge_sends[t][1 - i].wait_recv()
                joined[i, :, c] = (share[at(dest, block), c].astype(F32) + comb[i, :, c].astype(F32)).astype(BF16)
                cross_sends[t][1 - i].start()

    gd_sends = []

    def reduce_finish():
        for t in range(2):
            near_sends[t].wait_recv()
            cross_sends[t][0].wait_recv()
        total = acc[at(outer, block), :] + reduced[0].astype(F32) + reduced[1].astype(F32)
        final[...] = total.astype(BF16)
        for i, (q, d) in enumerate(others):
            gd_sends.append(go(final.at[at(q, rows), :], swapped.at[i], d))
        gd[:, at(me, part)] = final[at(me, rows), :].astype(F32)

    yes = outer >= 0
    own_down.wait()
    for c in swap_down:
        c.wait_recv()
    zstart(0, yes)
    for c in own_pair:
        c.wait()
    for c in swap_pair:
        c.wait_recv()
    for k in (1, 2):
        zforward(0, k)
        zarrive(0, k)
    for j in (1, 2):
        zstart(j, edge)
    zforward(0, 3)
    for j in (1, 2):
        zstart(j, middle)
    passes = {}
    x0.wait_recv()
    fy = go(piece(xn, 0), piece(xn, 0), ydev)
    passes["x", 0] = pass_on(xn, 0)
    y1.wait_recv()
    fx = go(piece(yn, 1), piece(yn, 1), xdev)
    passes["y", 1] = pass_on(yn, 1)
    arrive = {}
    saved = ((gate, gates), (up, ups))
    for name, cut, (q, d) in [("f", everything, others[0])] + [(n, c, o) for c in cuts for n, o in zip("xy", others[1:])]:
        arrive[name, cut] = [
            go(a.at[:, pl.ds(pl.multiple_of(q * part + cut[0], LANES), cut[1])], b.at[mine_of, pl.ds(*cut)], d)
            for a, b in saved
        ]
    own_cot.wait()
    own_gate.wait()
    own_up.wait()
    zarrive(0, 3)
    d_hidden(me)
    pointwise(me, everything)
    outer_product(me, everything, first=True)
    x1.wait_recv()
    passes["x", 1] = pass_on(xn, 1)
    y0.wait_recv()
    passes["y", 0] = pass_on(yn, 0)
    for j in (1, 2):
        for k in (1, 2):
            zforward(j, k)
    fy.wait_recv()
    passes["f", 0] = pass_on(far, 0)
    fx.wait_recv()
    passes["f", 1] = pass_on(far, 1)
    zforward(1, 3)
    for name, owner in (("x", xn), ("y", yn), ("f", far)):
        for i in range(2):
            passes[name, i].wait_recv()
        d_hidden(owner)
        if name == "y":
            zforward(2, 3)

    for c in arrive["f", everything]:
        c.wait_recv()
    pointwise(far, everything)
    for j in (1, 2):
        zarrive(j, 1)
    give_away(0, 0, far)
    keep_own(0, 0, far)
    give_away(0, 3, me)
    join(0, 0)
    send_far(0)
    outer_product(far, everything)
    keep_own(0, 3, me)
    join(0, 3)
    for name, owner in (("x", xn), ("y", yn)):
        for c in arrive[name, cuts[0]]:
            c.wait_recv()
        pointwise(owner, cuts[0])
        outer_product(owner, cuts[0], last=name == "y")
    reduce_start(0)
    for c in arrive["x", cuts[1]]:
        c.wait_recv()
    pointwise(xn, cuts[1])
    give_away(0, 1, xn)
    keep_own(0, 1, xn)
    for c in arrive["y", cuts[1]]:
        c.wait_recv()
    pointwise(yn, cuts[1])
    give_away(0, 2, yn)
    join(0, 1)
    send_x(0)
    keep_own(0, 2, yn)
    join(0, 2)
    send_y(0)
    outer_product(xn, cuts[1])
    relay(0)
    outer_product(yn, cuts[1], last=True)
    reduce_start(1)
    for k in (2, 3):
        for j in (1, 2):
            zarrive(j, k)
    give_away(1, 0, far)
    keep_own(1, 0, far)
    give_away(1, 1, xn)
    join(1, 0)
    send_far(1)
    reduce_join(0)
    keep_own(1, 1, xn)
    give_away(1, 2, yn)
    join(1, 1)
    send_x(1)
    keep_own(1, 2, yn)
    give_away(1, 3, me)
    join(1, 2)
    send_y(1)
    keep_own(1, 3, me)
    join(1, 3)
    reduce_join(1)
    finish(0)
    relay(1)
    reduce_finish()
    finish(1)
    for i, (q, _) in enumerate(others):
        gd_sends[i].wait_recv()
        gd[:, at(q, part)] = swapped[i].astype(F32)
    for c in lasts:
        c.wait_recv()
    for c in started:
        c.wait_send()
    for j in range(3):
        for cond, c in zown(j):

            @pl.when(cond)
            def _():
                c.wait_send()

    @pl.when(middle)
    def _():
        for j in range(3):
            for k in (1, 2, 3):
                zcopy(j, k).wait_send()
        for c in cross_sends[0] + cross_sends[1]:
            c.wait_send()

    @pl.when(edge)
    def _():
        for c in edge_sends[0] + edge_sends[1]:
            c.wait_send()

    for c in near_sends:
        c.wait_send()


def layer(gate_pre, up_pre, cotangent, gate_weight, up_weight, down_weight):
    tokens, width = gate_pre.shape
    rows, depth = gate_weight.shape[0], cotangent.shape[1]
    g = GROUP
    part, block, everyone = width // g, rows * g, tokens * g
    lane, half = block // 2, tokens // 2
    sems, vmem = pltpu.SemaphoreType.DMA, pltpu.VMEM
    struct = jax.ShapeDtypeStruct
    hbm = pl.BlockSpec(memory_space=pl.ANY)
    whole = pl.BlockSpec(memory_space=pltpu.VMEM)
    n = 72
    return pl.pallas_call(
        layer_kernel,
        out_shape=[vmem((tokens, depth), BF16), vmem((rows, width), F32)],
        in_specs=[hbm] * 6,
        out_specs=[whole] * 2,
        scratch_shapes=[
            vmem((everyone, depth), BF16),
            vmem((depth, part), BF16),
            vmem((depth, 2 * part), BF16),
            vmem((everyone, part), BF16),
            vmem((everyone, part), BF16),
            vmem((everyone, part), F32),
            vmem((everyone, part), BF16),
            vmem((everyone, 2 * part), BF16),
            vmem((depth, part), F32),
            vmem((depth, part), BF16),
            vmem((PARTS * 4, tokens, 2 * lane), BF16),
            vmem((PARTS * 4, tokens, 2 * lane), BF16),
            vmem((PARTS * 4, tokens, 2 * lane), BF16),
            vmem((PARTS, 2, tokens, 2 * lane), BF16),
            vmem((PARTS, 2, half, 2 * lane), BF16),
            vmem((2, block, part), BF16),
            vmem((2, block, part), BF16),
            vmem((2, block, part), BF16),
            vmem((block, part), BF16),
            vmem((3, rows, part), BF16),
            sems((n,)), sems((n,)), sems((3, 5)), sems((3, OUTER)), sems((2, 3)), sems((2, 4)), sems((6,)),
        ],
        compiler_params=pltpu.CompilerParams(
            collective_id=0, has_side_effects=True, vmem_limit_bytes=VMEM_LIMIT
        ),
    )(cotangent, gate_pre, up_pre, gate_weight, up_weight, down_weight)


def plain(gate_pre, up_pre, cotangent, gate_weight, up_weight, down_weight):
    gate = gate_pre.astype(F32)
    upper = up_pre.astype(F32)
    sigma = jax.nn.sigmoid(gate)
    hidden = (gate * sigma * upper).astype(BF16)
    share = lax.dot_general(cotangent, hidden, DOWN, preferred_element_type=F32)
    grad_down = lax.psum_scatter(share, "fs", scatter_dimension=0, tiled=True)
    d_hidden = jnp.dot(cotangent, lax.all_gather(down_weight, "fs", axis=0, tiled=True), preferred_element_type=F32)
    d_gate = (d_hidden * upper * sigma * (1.0 + gate * (1.0 - sigma))).astype(BF16)
    d_up = (d_hidden * gate * sigma).astype(BF16)
    gate_w, up_w = lax.all_gather((gate_weight, up_weight), "fs", axis=0, tiled=True)
    partial_sum = lax.dot_general(d_gate, gate_w, OVER, preferred_element_type=F32)
    partial_sum = partial_sum + lax.dot_general(d_up, up_w, OVER, preferred_element_type=F32)
    grad_input = lax.psum(partial_sum.astype(BF16), "tp").astype(F32).astype(BF16)
    return grad_input, grad_down


def solution(mesh):
    n_fs, n_tp = mesh.shape["fs"], mesh.shape["tp"]

    def local(*args):
        tokens, width = args[0].shape
        rows, depth = args[3].shape[0], args[2].shape[1]
        fits = n_tp == 2 and n_fs == GROUP * OUTER and width % (GROUP * LANES) == 0 and width >= 2 * GROUP * LANES
        fits = fits and rows % 64 == 0 and tokens % 512 == 0 and depth == rows * n_fs
        return layer(*args) if fits else plain(*args)

    both, rows = P("fs", "tp"), P("fs", None)
    return jax.shard_map(
        local, mesh=mesh, in_specs=(both, both, rows, both, both, both), out_specs=(rows, both), check_vma=False
    )
```

```python
import functools

import jax
import jax.numpy as jnp
from jax import lax
from jax.experimental import pallas as pl
from jax.experimental.pallas import tpu as pltpu
from jax.sharding import PartitionSpec as P

MESH = pl.DeviceIdType.MESH
F32, BF16 = jnp.float32, jnp.bfloat16
LANES = 128
VMEM_LIMIT = 58 * 1024 * 1024
GROUP, OUTER, PARTS = 4, 4, 2
OVER = (((1,), (1,)), ((), ()))
DOWN = (((0,), (0,)), ((), ()))


def at(index, size):
    return pl.ds(pl.multiple_of(index * size, size), size)


def remote(src, dst, send, recv, device):
    return pltpu.make_async_remote_copy(
        src_ref=src, dst_ref=dst, send_sem=send, recv_sem=recv, device_id=device, device_id_type=MESH
    )


def layer_kernel(
    cot, gate, up, gate_w, up_w, down_w, out, gd,
    cots, downs, pair_w, gates, ups, dh, hidden, dpair, acc, share,
    give, sib, mine, got, halves, comb, joined, reduced, final, swapped,
    send, recv, zsend, zrecv, rsend, rrecv, own, ready,
):
    g = GROUP
    fs, core = lax.axis_index("fs"), lax.axis_index("tp")
    outer, me = lax.div(fs, g), lax.rem(fs, g)
    base = outer * g
    x, y = lax.rem(me, 2), lax.div(me, 2)
    xn, yn, far = y * 2 + (1 - x), (1 - y) * 2 + x, 3 - me
    xdev, ydev, fdev, sibling = (base + xn, core), (base + yn, core), (base + far, core), (fs, 1 - core)
    others = [(far, fdev), (xn, xdev), (yn, ydev)]
    level = lambda o: (o * g + me, core)
    tokens, depth = cot.shape
    rows, part = down_w.shape[0], downs.shape[1]
    block = rows * g
    half, wide = tokens // 2, depth // 2
    edge = (outer == 0) | (outer == OUTER - 1)
    middle = jnp.logical_not(edge)
    low = outer < OUTER // 2

    above, below = level(jnp.minimum(outer + 1, OUTER - 1)), level(jnp.maximum(outer - 1, 0))

    def hello(semaphore, device):
        pl.semaphore_signal(semaphore, inc=1, device_id=device, device_id_type=MESH)

    barrier = pltpu.get_barrier_semaphore()
    for device in (xdev, ydev, sibling):
        hello(barrier, device)

    @pl.when(outer < OUTER - 1)
    def _():
        hello(barrier, above)

    @pl.when(outer > 0)
    def _():
        hello(barrier, below)

    pl.semaphore_wait(barrier, jnp.where(edge, 4, 5))
    hello(ready, xdev)

    started, count = [], [0]

    def go(src, dst, device):
        n = count[0]
        count[0] += 1
        c = remote(src, dst, send.at[n], recv.at[n], device)
        c.start()
        started.append(c)
        return c

    local = []

    def keep_local(src, dst):
        c = pltpu.make_async_copy(src, dst, own.at[len(local)])
        c.start()
        local.append(c)
        return c

    place = at(fs, rows)
    sides = [pl.ds(0, part), pl.ds(part, part)]
    near_down = [go(down_w.at[:, at(q, part)], downs.at[place, :], d) for q, d in others[1:]]
    pl.semaphore_wait(ready, 1)
    swap_down = [go(down_w.at[:, at(far, part)], downs.at[place, :], fdev)] + near_down
    own_down = keep_local(down_w.at[:, at(me, part)], downs.at[place, :])
    swap_pair = []
    own_pair = []
    for w, side in ((gate_w, sides[0]), (up_w, sides[1])):
        swap_pair += [go(w.at[:, at(q, part)], pair_w.at[place, side], d) for q, d in others]
        own_pair.append(keep_local(w.at[:, at(me, part)], pair_w.at[place, side]))

    cols = [pl.ds(0, wide), pl.ds(wide, wide)]
    piece = lambda owner, i: cots.at[at(owner * 2 + core, half), cols[i]]
    row_half = at(core, half)
    x0 = go(cot.at[row_half, cols[0]], piece(me, 0), xdev)
    y1 = go(cot.at[row_half, cols[1]], piece(me, 1), ydev)
    x1 = go(cot.at[row_half, cols[1]], piece(me, 1), xdev)
    y0 = go(cot.at[row_half, cols[0]], piece(me, 0), ydev)
    own_cot = keep_local(cot, cots.at[at(me, tokens), :])
    mine_of = at(me, tokens)
    own_gate = keep_local(gate.at[:, at(me, part)], gates.at[mine_of, :])
    own_up = keep_local(up.at[:, at(me, part)], ups.at[mine_of, :])

    def pass_on(owner, i):
        return go(piece(owner, i), piece(owner, i), sibling)

    def zblock(j, b):
        if j == 0:
            return downs.at[at(b, block), :]
        return pair_w.at[at(b * 2 + (j - 1), block // 2), :]

    def nearest(k):
        a = jnp.where(edge, k, (1, 2, 0, 3)[k])
        return jnp.where(low, a, OUTER - 1 - a)

    def zown(j):
        b = zblock(j, outer)
        return [
            (outer < OUTER - 1, remote(b, b, zsend.at[j, 0], zrecv.at[j, outer], above)),
            (outer > 0, remote(b, b, zsend.at[j, 1], zrecv.at[j, outer], below)),
        ]

    line_sends = []

    def zstart(j, only):
        for cond, c in zown(j):

            @pl.when(cond & only)
            def _():
                c.start()

    def zcopy(j, k):
        b = nearest(k)
        target = level(jnp.clip(jnp.where(b > outer, outer - 1, outer + 1), 0, OUTER - 1))
        return remote(zblock(j, b), zblock(j, b), zsend.at[j, 1 + k], zrecv.at[j, b], target)

    def zforward(j, k):
        c = zcopy(j, k)

        @pl.when(middle)
        def _():
            c.wait_recv()
            c.start()

    def zarrive(j, k):
        c = zcopy(j, k)

        @pl.when(edge)
        def _():
            c.wait_recv()

    tile = tokens // 2

    def d_hidden(owner):
        def step(i, carry):
            r = at(owner * 2 + i, tile)
            dh[r, :] = jnp.dot(cots[r, :], downs[...], preferred_element_type=F32)
            return carry

        lax.fori_loop(0, 2, step, 0)

    strip = tokens // 16
    first_cut = part // LANES * 2 // 3 * LANES
    cuts, everything = [(0, first_cut), (first_cut, part - first_cut)], (0, part)

    def pointwise(owner, cut):
        c, second = pl.ds(*cut), pl.ds(part + cut[0], cut[1])

        def step(i, carry):
            r = at(owner * 16 + i, strip)
            gv, uv, dv = gates[r, c].astype(F32), ups[r, c].astype(F32), dh[r, c]
            s = jax.nn.sigmoid(gv)
            gs = gv * s
            hidden[r, c] = (gs * uv).astype(BF16)
            dpair[r, c] = (dv * uv * s * (1.0 + gv * (1.0 - s))).astype(BF16)
            dpair[r, second] = (dv * gs).astype(BF16)
            return carry

        lax.fori_loop(0, 16, step, 0)

    span = depth // 8

    def outer_product(owner, cut, first=False, last=False):
        r, c = at(owner, tokens), pl.ds(*cut)

        def step(i, carry):
            d = at(i, span)
            new = lax.dot_general(cots[r, d], hidden[r, c], DOWN, preferred_element_type=F32)
            if not first:
                new = new + acc[d, c]
            acc[d, c] = new
            if last:
                share[d, c] = new.astype(BF16)
            return carry

        lax.fori_loop(0, 8, step, 0)

    lane = block // 2

    def product(p, owner, side, dst):
        r = at(owner, tokens)

        def step(i, carry):
            b = jnp.where(i == 0, nearest(2 * p), nearest(2 * p + 1))
            total = lax.dot_general(
                dpair[r, :], pair_w[at(b * 2 + side, lane), :], OVER, preferred_element_type=F32
            )
            dst[:, at(i, lane)] = total.astype(BF16)
            return carry

        lax.fori_loop(0, 2, step, 0)

    def add(dst, where, src):
        dst[where, :] = (dst[where, :].astype(F32) + src[...].astype(F32)).astype(BF16)

    slot = {}

    def give_away(p, n, owner):
        k = p * 4 + n
        product(p, owner, 1 - core, give.at[k])
        slot[k] = go(give.at[k], sib.at[k], sibling)

    def keep_own(p, n, owner):
        product(p, owner, core, mine.at[p * 4 + n])

    def join(p, n):
        k = p * 4 + n
        slot[k].wait_recv()
        add(mine.at[k], pl.ds(0, tokens), sib.at[k])

    top, bottom = pl.ds(0, half), pl.ds(half, half)
    crossing, arrivals = {}, {}

    def send_far(p):
        k = p * 4
        crossing[p, 0] = go(mine.at[k, top, :], halves.at[p, 0], xdev)
        crossing[p, 1] = go(mine.at[k, bottom, :], halves.at[p, 1], ydev)

    def send_x(p):
        arrivals[p, 0] = go(mine.at[p * 4 + 1, top, :], got.at[p, 0, top, :], xdev)

    def send_y(p):
        arrivals[p, 1] = go(mine.at[p * 4 + 2, bottom, :], got.at[p, 1, bottom, :], ydev)

    def relay(p):
        crossing[p, 1].wait_recv()
        add(mine.at[p * 4 + 1], bottom, halves.at[p, 1])
        arrivals[p, 2] = go(mine.at[p * 4 + 1, bottom, :], got.at[p, 0, bottom, :], xdev)
        crossing[p, 0].wait_recv()
        add(mine.at[p * 4 + 2], top, halves.at[p, 0])
        arrivals[p, 3] = go(mine.at[p * 4 + 2, top, :], got.at[p, 1, top, :], ydev)

    lasts = []

    def finish(p):
        for i in range(4):
            arrivals[p, i].wait_recv()
        for i in range(2):
            c = pl.ds(i * lane, lane)
            total = mine[p * 4 + 3, :, c].astype(F32) + got[p, 0, :, c].astype(F32) + got[p, 1, :, c].astype(F32)
            where = at(nearest(2 * p + i) * 2 + core, lane)
            out[:, where] = total.astype(BF16)
            lasts.append(go(out.at[:, where], out.at[:, where], sibling))

    near = jnp.where(low, 1 - outer, 5 - outer)
    cross_mid = jnp.where(low, 2, 1)
    cross_edge = jnp.where(low, 3, 0)
    edge_sends, near_sends, cross_sends = [], [], []
    for t, cut in enumerate(cuts):
        c = pl.ds(*cut)
        edge_sends.append([
            remote(share.at[at(cross_edge, block), c], comb.at[1, :, c], rsend.at[t, 0], rrecv.at[t, 0], level(near)),
            remote(share.at[at(cross_mid, block), c], comb.at[0, :, c], rsend.at[t, 1], rrecv.at[t, 1], level(near)),
        ])
        near_sends.append(
            remote(share.at[at(near, block), c], reduced.at[0, :, c], rsend.at[t, 2], rrecv.at[t, 2], level(near))
        )
        cross_sends.append([
            remote(joined.at[1, :, c], reduced.at[1, :, c], rsend.at[t, 0], rrecv.at[t, 3], level(cross_edge)),
            remote(joined.at[0, :, c], reduced.at[1, :, c], rsend.at[t, 1], rrecv.at[t, 3], level(cross_mid)),
        ])

    def reduce_start(t):
        @pl.when(edge)
        def _():
            for c in edge_sends[t]:
                c.start()

        near_sends[t].start()

    def reduce_join(t):
        c = pl.ds(*cuts[t])

        @pl.when(middle)
        def _():
            for i, dest in ((1, cross_edge), (0, cross_mid)):
                edge_sends[t][1 - i].wait_recv()
                joined[i, :, c] = (share[at(dest, block), c].astype(F32) + comb[i, :, c].astype(F32)).astype(BF16)
                cross_sends[t][1 - i].start()

    gd_sends = []

    def reduce_finish():
        for t in range(2):
            near_sends[t].wait_recv()
            cross_sends[t][0].wait_recv()
        total = acc[at(outer, block), :] + reduced[0].astype(F32) + reduced[1].astype(F32)
        final[...] = total.astype(BF16)
        for i, (q, d) in enumerate(others):
            gd_sends.append(go(final.at[at(q, rows), :], swapped.at[i], d))
        gd[:, at(me, part)] = final[at(me, rows), :].astype(F32)

    yes = outer >= 0
    own_down.wait()
    for c in swap_down:
        c.wait_recv()
    zstart(0, yes)
    for c in own_pair:
        c.wait()
    for c in swap_pair:
        c.wait_recv()
    for k in (1, 2):
        zforward(0, k)
        zarrive(0, k)
    for j in (1, 2):
        zstart(j, edge)
    zforward(0, 3)
    for j in (1, 2):
        zstart(j, middle)
    passes = {}
    x0.wait_recv()
    fy = go(piece(xn, 0), piece(xn, 0), ydev)
    passes["x", 0] = pass_on(xn, 0)
    y1.wait_recv()
    fx = go(piece(yn, 1), piece(yn, 1), xdev)
    passes["y", 1] = pass_on(yn, 1)
    arrive = {}
    saved = ((gate, gates), (up, ups))
    for name, cut, (q, d) in [("f", everything, others[0])] + [(n, c, o) for c in cuts for n, o in zip("xy", others[1:])]:
        arrive[name, cut] = [
            go(a.at[:, pl.ds(pl.multiple_of(q * part + cut[0], LANES), cut[1])], b.at[mine_of, pl.ds(*cut)], d)
            for a, b in saved
        ]
    own_cot.wait()
    own_gate.wait()
    own_up.wait()
    zarrive(0, 3)
    d_hidden(me)
    pointwise(me, everything)
    outer_product(me, everything, first=True)
    x1.wait_recv()
    passes["x", 1] = pass_on(xn, 1)
    y0.wait_recv()
    passes["y", 0] = pass_on(yn, 0)
    for j in (1, 2):
        for k in (1, 2):
            zforward(j, k)
    fy.wait_recv()
    passes["f", 0] = pass_on(far, 0)
    fx.wait_recv()
    passes["f", 1] = pass_on(far, 1)
    zforward(1, 3)
    for name, owner in (("x", xn), ("y", yn), ("f", far)):
        for i in range(2):
            passes[name, i].wait_recv()
        d_hidden(owner)
        if name == "y":
            zforward(2, 3)

    for c in arrive["f", everything]:
        c.wait_recv()
    pointwise(far, everything)
    for j in (1, 2):
        zarrive(j, 1)
    give_away(0, 0, far)
    keep_own(0, 0, far)
    give_away(0, 3, me)
    join(0, 0)
    send_far(0)
    outer_product(far, everything)
    keep_own(0, 3, me)
    join(0, 3)
    for name, owner in (("x", xn), ("y", yn)):
        for c in arrive[name, cuts[0]]:
            c.wait_recv()
        pointwise(owner, cuts[0])
        outer_product(owner, cuts[0], last=name == "y")
    reduce_start(0)
    for c in arrive["x", cuts[1]]:
        c.wait_recv()
    pointwise(xn, cuts[1])
    give_away(0, 1, xn)
    keep_own(0, 1, xn)
    for c in arrive["y", cuts[1]]:
        c.wait_recv()
    pointwise(yn, cuts[1])
    give_away(0, 2, yn)
    join(0, 1)
    send_x(0)
    keep_own(0, 2, yn)
    join(0, 2)
    send_y(0)
    outer_product(xn, cuts[1])
    relay(0)
    outer_product(yn, cuts[1], last=True)
    reduce_start(1)
    for k in (2, 3):
        for j in (1, 2):
            zarrive(j, k)
    give_away(1, 0, far)
    keep_own(1, 0, far)
    give_away(1, 1, xn)
    join(1, 0)
    send_far(1)
    reduce_join(0)
    keep_own(1, 1, xn)
    give_away(1, 2, yn)
    join(1, 1)
    send_x(1)
    keep_own(1, 2, yn)
    give_away(1, 3, me)
    join(1, 2)
    send_y(1)
    keep_own(1, 3, me)
    join(1, 3)
    reduce_join(1)
    finish(0)
    relay(1)
    reduce_finish()
    finish(1)
    for i, (q, _) in enumerate(others):
        gd_sends[i].wait_recv()
        gd[:, at(q, part)] = swapped[i].astype(F32)
    for c in lasts:
        c.wait_recv()
    for c in started:
        c.wait_send()
    for j in range(3):
        for cond, c in zown(j):

            @pl.when(cond)
            def _():
                c.wait_send()

    @pl.when(middle)
    def _():
        for j in range(3):
            for k in (1, 2, 3):
                zcopy(j, k).wait_send()
        for c in cross_sends[0] + cross_sends[1]:
            c.wait_send()

    @pl.when(edge)
    def _():
        for c in edge_sends[0] + edge_sends[1]:
            c.wait_send()

    for c in near_sends:
        c.wait_send()


def flush_kernel(a, b, out_a, out_b, sems):
    copies = []
    for src, dst, pieces in ((a, out_a, 4), (b, out_b, 2)):
        rows = src.shape[0] // pieces
        for i in range(pieces):
            r = pl.ds(i * rows, rows)
            copies.append(pltpu.make_async_copy(src.at[r, :], dst.at[r, :], sems.at[len(copies)]))
    for c in copies:
        c.start()
    for c in copies:
        c.wait()


def layer(gate_pre, up_pre, cotangent, gate_weight, up_weight, down_weight):
    tokens, width = gate_pre.shape
    rows, depth = gate_weight.shape[0], cotangent.shape[1]
    g = GROUP
    part, block, everyone = width // g, rows * g, tokens * g
    lane, half = block // 2, tokens // 2
    sems, vmem = pltpu.SemaphoreType.DMA, pltpu.VMEM
    struct = jax.ShapeDtypeStruct
    hbm = pl.BlockSpec(memory_space=pl.ANY)
    whole = pl.BlockSpec(memory_space=pltpu.VMEM)
    n = 72
    made = pl.pallas_call(
        layer_kernel,
        out_shape=[vmem((tokens, depth), BF16), vmem((rows, width), F32)],
        in_specs=[hbm] * 6,
        out_specs=[whole] * 2,
        scratch_shapes=[
            vmem((everyone, depth), BF16),
            vmem((depth, part), BF16),
            vmem((depth, 2 * part), BF16),
            vmem((everyone, part), BF16),
            vmem((everyone, part), BF16),
            vmem((everyone, part), F32),
            vmem((everyone, part), BF16),
            vmem((everyone, 2 * part), BF16),
            vmem((depth, part), F32),
            vmem((depth, part), BF16),
            vmem((PARTS * 4, tokens, 2 * lane), BF16),
            vmem((PARTS * 4, tokens, 2 * lane), BF16),
            vmem((PARTS * 4, tokens, 2 * lane), BF16),
            vmem((PARTS, 2, tokens, 2 * lane), BF16),
            vmem((PARTS, 2, half, 2 * lane), BF16),
            vmem((2, block, part), BF16),
            vmem((2, block, part), BF16),
            vmem((2, block, part), BF16),
            vmem((block, part), BF16),
            vmem((3, rows, part), BF16),
            sems((n,)), sems((n,)), sems((3, 5)), sems((3, OUTER)), sems((2, 3)), sems((2, 4)), sems((6,)),
            pltpu.SemaphoreType.REGULAR,
        ],
        compiler_params=pltpu.CompilerParams(
            collective_id=0, has_side_effects=True, vmem_limit_bytes=VMEM_LIMIT
        ),
    )(cotangent, gate_pre, up_pre, gate_weight, up_weight, down_weight)
    return pl.pallas_call(
        flush_kernel,
        out_shape=[struct((tokens, depth), BF16), struct((rows, width), F32)],
        in_specs=[whole] * 2,
        out_specs=[hbm] * 2,
        scratch_shapes=[sems((6,))],
        compiler_params=pltpu.CompilerParams(vmem_limit_bytes=4 * 1024 * 1024),
    )(*[pltpu.with_memory_space_constraint(m, pltpu.VMEM) for m in made])


def plain(gate_pre, up_pre, cotangent, gate_weight, up_weight, down_weight):
    gate = gate_pre.astype(F32)
    upper = up_pre.astype(F32)
    sigma = jax.nn.sigmoid(gate)
    hidden = (gate * sigma * upper).astype(BF16)
    share = lax.dot_general(cotangent, hidden, DOWN, preferred_element_type=F32)
    grad_down = lax.psum_scatter(share, "fs", scatter_dimension=0, tiled=True)
    d_hidden = jnp.dot(cotangent, lax.all_gather(down_weight, "fs", axis=0, tiled=True), preferred_element_type=F32)
    d_gate = (d_hidden * upper * sigma * (1.0 + gate * (1.0 - sigma))).astype(BF16)
    d_up = (d_hidden * gate * sigma).astype(BF16)
    gate_w, up_w = lax.all_gather((gate_weight, up_weight), "fs", axis=0, tiled=True)
    partial_sum = lax.dot_general(d_gate, gate_w, OVER, preferred_element_type=F32)
    partial_sum = partial_sum + lax.dot_general(d_up, up_w, OVER, preferred_element_type=F32)
    grad_input = lax.psum(partial_sum.astype(BF16), "tp").astype(F32).astype(BF16)
    return grad_input, grad_down


def solution(mesh):
    n_fs, n_tp = mesh.shape["fs"], mesh.shape["tp"]

    def local(*args):
        tokens, width = args[0].shape
        rows, depth = args[3].shape[0], args[2].shape[1]
        fits = n_tp == 2 and n_fs == GROUP * OUTER and width % (GROUP * LANES) == 0 and width >= 2 * GROUP * LANES
        fits = fits and rows % 64 == 0 and tokens % 512 == 0 and depth == rows * n_fs
        return layer(*args) if fits else plain(*args)

    both, rows = P("fs", "tp"), P("fs", None)
    return jax.shard_map(
        local, mesh=mesh, in_specs=(both, both, rows, both, both, both), out_specs=(rows, both), check_vma=False
    )
```

```python
import functools

import jax
import jax.numpy as jnp
from jax import lax
from jax.experimental import pallas as pl
from jax.experimental.pallas import tpu as pltpu
from jax.sharding import PartitionSpec as P

MESH = pl.DeviceIdType.MESH
F32, BF16 = jnp.float32, jnp.bfloat16
LANES = 128
VMEM_LIMIT = 58 * 1024 * 1024
GROUP, OUTER, PARTS = 4, 4, 2
SEND_SLOTS, RECV_SLOTS = 21, 58
OVER = (((1,), (1,)), ((), ()))
DOWN = (((0,), (0,)), ((), ()))


def at(index, size):
    return pl.ds(pl.multiple_of(index * size, size), size)


def remote(src, dst, send, recv, device):
    return pltpu.make_async_remote_copy(
        src_ref=src, dst_ref=dst, send_sem=send, recv_sem=recv, device_id=device, device_id_type=MESH
    )


def layer_kernel(
    cot, gate, up, gate_w, up_w, down_w, out, gd,
    cots, downs, pair_w, gates, ups, dh, hidden, dpair, acc, share,
    give, sib, mine, got, halves, comb, joined, reduced, final, swapped, stage,
    send, recv, zsend, zrecv, rsend, rrecv, own, ready,
):
    g = GROUP
    fs, core = lax.axis_index("fs"), lax.axis_index("tp")
    outer, me = lax.div(fs, g), lax.rem(fs, g)
    base = outer * g
    x, y = lax.rem(me, 2), lax.div(me, 2)
    xn, yn, far = y * 2 + (1 - x), (1 - y) * 2 + x, 3 - me
    xdev, ydev, fdev, sibling = (base + xn, core), (base + yn, core), (base + far, core), (fs, 1 - core)
    others = [(far, fdev), (xn, xdev), (yn, ydev)]
    level = lambda o: (o * g + me, core)
    tokens, depth = cot.shape
    rows, part = down_w.shape[0], downs.shape[1]
    block = rows * g
    half, wide = tokens // 2, depth // 2
    edge = (outer == 0) | (outer == OUTER - 1)
    middle = jnp.logical_not(edge)
    low = outer < OUTER // 2

    above, below = level(jnp.minimum(outer + 1, OUTER - 1)), level(jnp.maximum(outer - 1, 0))

    def hello(semaphore, device):
        pl.semaphore_signal(semaphore, inc=1, device_id=device, device_id_type=MESH)

    staged = pltpu.make_async_copy(down_w, stage, own.at[6])
    staged.start()

    barrier = pltpu.get_barrier_semaphore()
    for device in (xdev, ydev, sibling):
        hello(barrier, device)

    @pl.when(outer < OUTER - 1)
    def _():
        hello(barrier, above)

    @pl.when(outer > 0)
    def _():
        hello(barrier, below)

    pl.semaphore_wait(barrier, jnp.where(edge, 4, 5))
    hello(ready, xdev)

    started, free, count = {}, list(range(SEND_SLOTS)), [0]

    def go(src, dst, device):
        slot, n = free.pop(0), count[0]
        count[0] += 1
        c = remote(src, dst, send.at[slot], recv.at[n], device)
        c.start()
        started[id(c)] = (c, slot)
        return c

    def retire(*copies):
        for c in copies:
            c.wait_send()
            free.append(started.pop(id(c))[1])

    local = []

    def keep_local(src, dst):
        c = pltpu.make_async_copy(src, dst, own.at[len(local)])
        c.start()
        local.append(c)
        return c

    place = at(fs, rows)
    sides = [pl.ds(0, part), pl.ds(part, part)]
    staged.wait()
    near_down = [go(stage.at[:, at(q, part)], downs.at[place, :], d) for q, d in others[1:]]
    pl.semaphore_wait(ready, 1)
    swap_down = [go(stage.at[:, at(far, part)], downs.at[place, :], fdev)] + near_down
    own_down = keep_local(stage.at[:, at(me, part)], downs.at[place, :])
    swap_pair = []
    own_pair = []
    for w, side in ((gate_w, sides[0]), (up_w, sides[1])):
        swap_pair += [go(w.at[:, at(q, part)], pair_w.at[place, side], d) for q, d in others]
        own_pair.append(keep_local(w.at[:, at(me, part)], pair_w.at[place, side]))

    cols = [pl.ds(0, wide), pl.ds(wide, wide)]
    piece = lambda owner, i: cots.at[at(owner * 2 + core, half), cols[i]]
    row_half = at(core, half)
    x0 = go(cot.at[row_half, cols[0]], piece(me, 0), xdev)
    y1 = go(cot.at[row_half, cols[1]], piece(me, 1), ydev)
    x1 = go(cot.at[row_half, cols[1]], piece(me, 1), xdev)
    y0 = go(cot.at[row_half, cols[0]], piece(me, 0), ydev)
    own_cot = keep_local(cot, cots.at[at(me, tokens), :])
    mine_of = at(me, tokens)
    own_gate = keep_local(gate.at[:, at(me, part)], gates.at[mine_of, :])
    own_up = keep_local(up.at[:, at(me, part)], ups.at[mine_of, :])

    def pass_on(owner, i):
        return go(piece(owner, i), piece(owner, i), sibling)

    def zblock(j, b):
        if j == 0:
            return downs.at[at(b, block), :]
        return pair_w.at[at(b * 2 + (j - 1), block // 2), :]

    def nearest(k):
        a = jnp.where(edge, k, (1, 2, 0, 3)[k])
        return jnp.where(low, a, OUTER - 1 - a)

    def zown(j):
        b = zblock(j, outer)
        return [
            (outer < OUTER - 1, remote(b, b, zsend.at[j % 2, 0], zrecv.at[j, outer], above)),
            (outer > 0, remote(b, b, zsend.at[j % 2, 1], zrecv.at[j, outer], below)),
        ]

    def zstart(j, only):
        for way, (cond, c) in enumerate(zown(j)):

            @pl.when(cond & only)
            def _():
                if j == 2:
                    zown(0)[way][1].wait_send()
                c.start()

    def zcopy(j, k):
        b = nearest(k)
        target = level(jnp.clip(jnp.where(b > outer, outer - 1, outer + 1), 0, OUTER - 1))
        return remote(zblock(j, b), zblock(j, b), zsend.at[j % 2, 1 + k], zrecv.at[j, b], target)

    def zforward(j, k):
        c = zcopy(j, k)

        @pl.when(middle)
        def _():
            c.wait_recv()
            if j == 2:
                zcopy(0, k).wait_send()
            c.start()

    def zarrive(j, k):
        c = zcopy(j, k)

        @pl.when(edge)
        def _():
            c.wait_recv()

    tile = tokens // 2

    def d_hidden(owner):
        def step(i, carry):
            r = at(owner * 2 + i, tile)
            dh[r, :] = jnp.dot(cots[r, :], downs[...], preferred_element_type=F32)
            return carry

        lax.fori_loop(0, 2, step, 0)

    strip = tokens // 16
    first_cut = part // LANES * 2 // 3 * LANES
    cuts, everything = [(0, first_cut), (first_cut, part - first_cut)], (0, part)

    def pointwise(owner, cut):
        c, second = pl.ds(*cut), pl.ds(part + cut[0], cut[1])

        def step(i, carry):
            r = at(owner * 16 + i, strip)
            gv, uv, dv = gates[r, c].astype(F32), ups[r, c].astype(F32), dh[r, c]
            s = jax.nn.sigmoid(gv)
            gs = gv * s
            hidden[r, c] = (gs * uv).astype(BF16)
            dpair[r, c] = (dv * uv * s * (1.0 + gv * (1.0 - s))).astype(BF16)
            dpair[r, second] = (dv * gs).astype(BF16)
            return carry

        lax.fori_loop(0, 16, step, 0)

    span = depth // 8

    def outer_product(owner, cut, first=False, last=False):
        r, c = at(owner, tokens), pl.ds(*cut)

        def step(i, carry):
            d = at(i, span)
            new = lax.dot_general(cots[r, d], hidden[r, c], DOWN, preferred_element_type=F32)
            if not first:
                new = new + acc[d, c]
            acc[d, c] = new
            if last:
                share[d, c] = new.astype(BF16)
            return carry

        lax.fori_loop(0, 8, step, 0)

    lane = block // 2

    def product(p, owner, side, dst):
        r = at(owner, tokens)

        def step(i, carry):
            b = jnp.where(i == 0, nearest(2 * p), nearest(2 * p + 1))
            total = lax.dot_general(
                dpair[r, :], pair_w[at(b * 2 + side, lane), :], OVER, preferred_element_type=F32
            )
            dst[:, at(i, lane)] = total.astype(BF16)
            return carry

        lax.fori_loop(0, 2, step, 0)

    def add(dst, where, src):
        dst[where, :] = (dst[where, :].astype(F32) + src[...].astype(F32)).astype(BF16)

    slot = {}

    def give_away(p, n, owner):
        k = p * 4 + n
        product(p, owner, 1 - core, give.at[k])
        slot[k] = go(give.at[k], sib.at[k], sibling)

    def keep_own(p, n, owner):
        product(p, owner, core, mine.at[p * 4 + n])

    def join(p, n):
        k = p * 4 + n
        slot[k].wait_recv()
        add(mine.at[k], pl.ds(0, tokens), sib.at[k])

    top, bottom = pl.ds(0, half), pl.ds(half, half)
    crossing, arrivals = {}, {}

    def send_far(p):
        k = p * 4
        crossing[p, 0] = go(mine.at[k, top, :], halves.at[p, 0], xdev)
        crossing[p, 1] = go(mine.at[k, bottom, :], halves.at[p, 1], ydev)

    def send_x(p):
        arrivals[p, 0] = go(mine.at[p * 4 + 1, top, :], got.at[p, 0, top, :], xdev)

    def send_y(p):
        arrivals[p, 1] = go(mine.at[p * 4 + 2, bottom, :], got.at[p, 1, bottom, :], ydev)

    def relay(p):
        crossing[p, 1].wait_recv()
        add(mine.at[p * 4 + 1], bottom, halves.at[p, 1])
        arrivals[p, 2] = go(mine.at[p * 4 + 1, bottom, :], got.at[p, 0, bottom, :], xdev)
        crossing[p, 0].wait_recv()
        add(mine.at[p * 4 + 2], top, halves.at[p, 0])
        arrivals[p, 3] = go(mine.at[p * 4 + 2, top, :], got.at[p, 1, top, :], ydev)

    lasts = []

    def finish(p):
        for i in range(4):
            arrivals[p, i].wait_recv()
        for i in range(2):
            c = pl.ds(i * lane, lane)
            total = mine[p * 4 + 3, :, c].astype(F32) + got[p, 0, :, c].astype(F32) + got[p, 1, :, c].astype(F32)
            where = at(nearest(2 * p + i) * 2 + core, lane)
            out[:, where] = total.astype(BF16)
            lasts.append(go(out.at[:, where], out.at[:, where], sibling))

    near = jnp.where(low, 1 - outer, 5 - outer)
    cross_mid = jnp.where(low, 2, 1)
    cross_edge = jnp.where(low, 3, 0)
    edge_sends, near_sends, cross_sends = [], [], []
    for t, cut in enumerate(cuts):
        c = pl.ds(*cut)
        edge_sends.append([
            remote(share.at[at(cross_edge, block), c], comb.at[1, :, c], rsend.at[t, 0], rrecv.at[t, 0], level(near)),
            remote(share.at[at(cross_mid, block), c], comb.at[0, :, c], rsend.at[t, 1], rrecv.at[t, 1], level(near)),
        ])
        near_sends.append(
            remote(share.at[at(near, block), c], reduced.at[0, :, c], rsend.at[t, 2], rrecv.at[t, 2], level(near))
        )
        cross_sends.append([
            remote(joined.at[1, :, c], reduced.at[1, :, c], rsend.at[t, 0], rrecv.at[t, 3], level(cross_edge)),
            remote(joined.at[0, :, c], reduced.at[1, :, c], rsend.at[t, 1], rrecv.at[t, 3], level(cross_mid)),
        ])

    def reduce_start(t):
        @pl.when(edge)
        def _():
            for c in edge_sends[t]:
                c.start()

        near_sends[t].start()

    def reduce_join(t):
        c = pl.ds(*cuts[t])

        @pl.when(middle)
        def _():
            for i, dest in ((1, cross_edge), (0, cross_mid)):
                edge_sends[t][1 - i].wait_recv()
                joined[i, :, c] = (share[at(dest, block), c].astype(F32) + comb[i, :, c].astype(F32)).astype(BF16)
                cross_sends[t][1 - i].start()

    gd_sends = {}

    def reduce_finish():
        for t in range(2):
            near_sends[t].wait_recv()
            cross_sends[t][0].wait_recv()
        total = acc[at(outer, block), :] + reduced[0].astype(F32) + reduced[1].astype(F32)
        final[...] = total.astype(BF16)
        for i in (2, 0, 1):
            q, d = others[i]
            gd_sends[i] = go(final.at[at(q, rows), :], swapped.at[i], d)
        gd[:, at(me, part)] = final[at(me, rows), :].astype(F32)

    yes = outer >= 0
    own_down.wait()
    for c in swap_down:
        c.wait_recv()
    zstart(0, yes)
    for c in own_pair:
        c.wait()
    for c in swap_pair:
        c.wait_recv()
    for k in (1, 2):
        zforward(0, k)
        zarrive(0, k)
    for j in (1, 2):
        zstart(j, edge)
    zforward(0, 3)
    for j in (1, 2):
        zstart(j, middle)
    retire(*swap_down, *swap_pair)
    passes = {}
    x0.wait_recv()
    fy = go(piece(xn, 0), piece(xn, 0), ydev)
    passes["x", 0] = pass_on(xn, 0)
    y1.wait_recv()
    fx = go(piece(yn, 1), piece(yn, 1), xdev)
    passes["y", 1] = pass_on(yn, 1)
    arrive = {}
    saved = ((gate, gates), (up, ups))
    for name, cut, (q, d) in [("f", everything, others[0])] + [(n, c, o) for c in cuts for n, o in zip("xy", others[1:])]:
        arrive[name, cut] = [
            go(a.at[:, pl.ds(pl.multiple_of(q * part + cut[0], LANES), cut[1])], b.at[mine_of, pl.ds(*cut)], d)
            for a, b in saved
        ]
    own_cot.wait()
    own_gate.wait()
    own_up.wait()
    zarrive(0, 3)
    d_hidden(me)
    pointwise(me, everything)
    outer_product(me, everything, first=True)
    x1.wait_recv()
    passes["x", 1] = pass_on(xn, 1)
    y0.wait_recv()
    passes["y", 0] = pass_on(yn, 0)
    for j in (1, 2):
        for k in (1, 2):
            zforward(j, k)
    retire(x0, y1, x1, y0)
    fy.wait_recv()
    passes["f", 0] = pass_on(far, 0)
    fx.wait_recv()
    passes["f", 1] = pass_on(far, 1)
    zforward(1, 3)
    for name, owner in (("x", xn), ("y", yn), ("f", far)):
        for i in range(2):
            passes[name, i].wait_recv()
        d_hidden(owner)
        if name == "y":
            zforward(2, 3)

    for c in arrive["f", everything]:
        c.wait_recv()
    retire(fy, fx, *passes.values())
    pointwise(far, everything)
    for j in (1, 2):
        zarrive(j, 1)
    give_away(0, 0, far)
    keep_own(0, 0, far)
    give_away(0, 3, me)
    join(0, 0)
    send_far(0)
    outer_product(far, everything)
    keep_own(0, 3, me)
    join(0, 3)
    for name, owner in (("x", xn), ("y", yn)):
        for c in arrive[name, cuts[0]]:
            c.wait_recv()
        pointwise(owner, cuts[0])
        outer_product(owner, cuts[0], last=name == "y")
    reduce_start(0)
    for c in arrive["x", cuts[1]]:
        c.wait_recv()
    pointwise(xn, cuts[1])
    give_away(0, 1, xn)
    keep_own(0, 1, xn)
    for c in arrive["y", cuts[1]]:
        c.wait_recv()
    pointwise(yn, cuts[1])
    give_away(0, 2, yn)
    join(0, 1)
    send_x(0)
    keep_own(0, 2, yn)
    join(0, 2)
    send_y(0)
    outer_product(xn, cuts[1])
    relay(0)
    outer_product(yn, cuts[1], last=True)
    reduce_start(1)
    retire(*[c for cs in arrive.values() for c in cs], *slot.values(), crossing[0, 0], crossing[0, 1])
    for k in (2, 3):
        for j in (1, 2):
            zarrive(j, k)
    give_away(1, 0, far)
    keep_own(1, 0, far)
    give_away(1, 1, xn)
    join(1, 0)
    send_far(1)
    reduce_join(0)
    keep_own(1, 1, xn)
    give_away(1, 2, yn)
    join(1, 1)
    send_x(1)
    keep_own(1, 2, yn)
    give_away(1, 3, me)
    join(1, 2)
    send_y(1)
    keep_own(1, 3, me)
    join(1, 3)
    reduce_join(1)
    finish(0)
    relay(1)
    reduce_finish()
    finish(1)
    for i, (q, _) in enumerate(others):
        gd_sends[i].wait_recv()
        gd[:, at(q, part)] = swapped[i].astype(F32)
    for c in lasts:
        c.wait_recv()
    retire(*[c for c, _ in started.values()])
    for j in (1, 2):
        for cond, c in zown(j):

            @pl.when(cond)
            def _():
                c.wait_send()

    @pl.when(middle)
    def _():
        for j in (1, 2):
            for k in (1, 2, 3):
                zcopy(j, k).wait_send()
        for c in cross_sends[0] + cross_sends[1]:
            c.wait_send()

    @pl.when(edge)
    def _():
        for c in edge_sends[0] + edge_sends[1]:
            c.wait_send()

    for c in near_sends:
        c.wait_send()


def flush_kernel(a, b, out_a, out_b, sems):
    copies = []
    for src, dst, pieces in ((a, out_a, 1), (b, out_b, 1)):
        rows = src.shape[0] // pieces
        for i in range(pieces):
            r = pl.ds(i * rows, rows)
            copies.append(pltpu.make_async_copy(src.at[r, :], dst.at[r, :], sems.at[len(copies)]))
    for c in copies:
        c.start()
    for c in copies:
        c.wait()


def layer(gate_pre, up_pre, cotangent, gate_weight, up_weight, down_weight):
    tokens, width = gate_pre.shape
    rows, depth = gate_weight.shape[0], cotangent.shape[1]
    g = GROUP
    part, block, everyone = width // g, rows * g, tokens * g
    lane, half = block // 2, tokens // 2
    sems, vmem = pltpu.SemaphoreType.DMA, pltpu.VMEM
    struct = jax.ShapeDtypeStruct
    hbm = pl.BlockSpec(memory_space=pl.ANY)
    whole = pl.BlockSpec(memory_space=pltpu.VMEM)
    made = pl.pallas_call(
        layer_kernel,
        out_shape=[vmem((tokens, depth), BF16), vmem((rows, width), F32)],
        in_specs=[hbm] * 6,
        out_specs=[whole] * 2,
        scratch_shapes=[
            vmem((everyone, depth), BF16),
            vmem((depth, part), BF16),
            vmem((depth, 2 * part), BF16),
            vmem((everyone, part), BF16),
            vmem((everyone, part), BF16),
            vmem((everyone, part), F32),
            vmem((everyone, part), BF16),
            vmem((everyone, 2 * part), BF16),
            vmem((depth, part), F32),
            vmem((depth, part), BF16),
            vmem((PARTS * 4, tokens, 2 * lane), BF16),
            vmem((PARTS * 4, tokens, 2 * lane), BF16),
            vmem((PARTS * 4, tokens, 2 * lane), BF16),
            vmem((PARTS, 2, tokens, 2 * lane), BF16),
            vmem((PARTS, 2, half, 2 * lane), BF16),
            vmem((2, block, part), BF16),
            vmem((2, block, part), BF16),
            vmem((2, block, part), BF16),
            vmem((block, part), BF16),
            vmem((3, rows, part), BF16),
            vmem((rows, width), BF16),
            sems((SEND_SLOTS,)), sems((RECV_SLOTS,)), sems((2, 5)), sems((3, OUTER)), sems((2, 3)), sems((2, 4)), sems((7,)),
            pltpu.SemaphoreType.REGULAR,
        ],
        compiler_params=pltpu.CompilerParams(
            collective_id=0, has_side_effects=True, vmem_limit_bytes=VMEM_LIMIT
        ),
    )(cotangent, gate_pre, up_pre, gate_weight, up_weight, down_weight)
    return pl.pallas_call(
        flush_kernel,
        out_shape=[struct((tokens, depth), BF16), struct((rows, width), F32)],
        in_specs=[whole] * 2,
        out_specs=[hbm] * 2,
        scratch_shapes=[sems((2,))],
        compiler_params=pltpu.CompilerParams(vmem_limit_bytes=4 * 1024 * 1024),
    )(*[pltpu.with_memory_space_constraint(m, pltpu.VMEM) for m in made])


def plain(gate_pre, up_pre, cotangent, gate_weight, up_weight, down_weight):
    gate = gate_pre.astype(F32)
    upper = up_pre.astype(F32)
    sigma = jax.nn.sigmoid(gate)
    hidden = (gate * sigma * upper).astype(BF16)
    share = lax.dot_general(cotangent, hidden, DOWN, preferred_element_type=F32)
    grad_down = lax.psum_scatter(share, "fs", scatter_dimension=0, tiled=True)
    d_hidden = jnp.dot(cotangent, lax.all_gather(down_weight, "fs", axis=0, tiled=True), preferred_element_type=F32)
    d_gate = (d_hidden * upper * sigma * (1.0 + gate * (1.0 - sigma))).astype(BF16)
    d_up = (d_hidden * gate * sigma).astype(BF16)
    gate_w, up_w = lax.all_gather((gate_weight, up_weight), "fs", axis=0, tiled=True)
    partial_sum = lax.dot_general(d_gate, gate_w, OVER, preferred_element_type=F32)
    partial_sum = partial_sum + lax.dot_general(d_up, up_w, OVER, preferred_element_type=F32)
    grad_input = lax.psum(partial_sum.astype(BF16), "tp").astype(F32).astype(BF16)
    return grad_input, grad_down


def solution(mesh):
    n_fs, n_tp = mesh.shape["fs"], mesh.shape["tp"]

    def local(*args):
        tokens, width = args[0].shape
        rows, depth = args[3].shape[0], args[2].shape[1]
        fits = n_tp == 2 and n_fs == GROUP * OUTER and width % (GROUP * LANES) == 0 and width >= 2 * GROUP * LANES
        fits = fits and rows % 64 == 0 and tokens % 512 == 0 and depth == rows * n_fs
        return layer(*args) if fits else plain(*args)

    both, rows = P("fs", "tp"), P("fs", None)
    return jax.shard_map(
        local, mesh=mesh, in_specs=(both, both, rows, both, both, both), out_specs=(rows, both), check_vma=False
    )
```

```python
import functools

import jax
import jax.numpy as jnp
from jax import lax
from jax.experimental import pallas as pl
from jax.experimental.pallas import tpu as pltpu
from jax.sharding import PartitionSpec as P

MESH = pl.DeviceIdType.MESH
F32, BF16 = jnp.float32, jnp.bfloat16
LANES = 128
VMEM_LIMIT = 58 * 1024 * 1024
GROUP, OUTER, PARTS = 4, 4, 2
SEND_SLOTS, RECV_SLOTS = 22, 60
OVER = (((1,), (1,)), ((), ()))
DOWN = (((0,), (0,)), ((), ()))


def at(index, size):
    return pl.ds(pl.multiple_of(index * size, size), size)


def remote(src, dst, send, recv, device):
    return pltpu.make_async_remote_copy(
        src_ref=src, dst_ref=dst, send_sem=send, recv_sem=recv, device_id=device, device_id_type=MESH
    )


def layer_kernel(
    cot, gate, up, gate_w, up_w, down_w, out, gd,
    cots, downs, pair_w, gates, ups, dh, hidden, dpair, acc, share,
    give, sib, mine, got, halves, comb, joined, reduced, final, swapped, turned, stage,
    send, recv, zsend, zrecv, rsend, rrecv, own, ready,
):
    g = GROUP
    fs, core = lax.axis_index("fs"), lax.axis_index("tp")
    outer, me = lax.div(fs, g), lax.rem(fs, g)
    base = outer * g
    x, y = lax.rem(me, 2), lax.div(me, 2)
    xn, yn, far = y * 2 + (1 - x), (1 - y) * 2 + x, 3 - me
    xdev, ydev, fdev, sibling = (base + xn, core), (base + yn, core), (base + far, core), (fs, 1 - core)
    others = [(far, fdev), (xn, xdev), (yn, ydev)]
    level = lambda o: (o * g + me, core)
    tokens, depth = cot.shape
    rows, part = down_w.shape[0], downs.shape[1]
    block = rows * g
    half, wide = tokens // 2, depth // 2
    edge = (outer == 0) | (outer == OUTER - 1)
    middle = jnp.logical_not(edge)
    low = outer < OUTER // 2

    above, below = level(jnp.minimum(outer + 1, OUTER - 1)), level(jnp.maximum(outer - 1, 0))

    def hello(semaphore, device):
        pl.semaphore_signal(semaphore, inc=1, device_id=device, device_id_type=MESH)

    staged = pltpu.make_async_copy(down_w, stage, own.at[6])
    staged.start()

    barrier = pltpu.get_barrier_semaphore()
    for device in (xdev, ydev, sibling):
        hello(barrier, device)

    @pl.when(outer < OUTER - 1)
    def _():
        hello(barrier, above)

    @pl.when(outer > 0)
    def _():
        hello(barrier, below)

    pl.semaphore_wait(barrier, jnp.where(edge, 4, 5))
    hello(ready, xdev)

    started, free, count = {}, list(range(SEND_SLOTS)), [0]

    def go(src, dst, device):
        slot, n = free.pop(0), count[0]
        count[0] += 1
        c = remote(src, dst, send.at[slot], recv.at[n], device)
        c.start()
        started[id(c)] = (c, slot)
        return c

    def retire(*copies):
        for c in copies:
            c.wait_send()
            free.append(started.pop(id(c))[1])

    local = []

    def keep_local(src, dst):
        c = pltpu.make_async_copy(src, dst, own.at[len(local)])
        c.start()
        local.append(c)
        return c

    place = at(fs, rows)
    sides = [pl.ds(0, part), pl.ds(part, part)]
    staged.wait()
    jobs = [(stage, downs, pl.ds(0, part)), (gate_w, pair_w, sides[0]), (up_w, pair_w, sides[1])]
    swaps = {}
    for n, (w, dst, side) in enumerate(jobs):
        for i, (q, d) in list(enumerate(others))[1:]:
            swaps[n, i] = go(w.at[:, at(q, part)], dst.at[place, side], d)
    pl.semaphore_wait(ready, 1)
    for n, (w, dst, side) in enumerate(jobs):
        swaps[n, 0] = go(w.at[:, at(far, part)], dst.at[place, side], fdev)
    swap_down = [swaps[0, i] for i in range(3)]
    swap_pair = [swaps[n, i] for n in (1, 2) for i in range(3)]
    own_down, *own_pair = [keep_local(w.at[:, at(me, part)], dst.at[place, side]) for w, dst, side in jobs]

    cols = [pl.ds(0, wide), pl.ds(wide, wide)]
    piece = lambda owner, i: cots.at[at(owner * 2 + core, half), cols[i]]
    row_half = at(core, half)
    x0 = go(cot.at[row_half, cols[0]], piece(me, 0), xdev)
    x1 = go(cot.at[row_half, cols[1]], piece(me, 1), xdev)
    own_cot = keep_local(cot, cots.at[at(me, tokens), :])
    mine_of = at(me, tokens)
    own_gate = keep_local(gate.at[:, at(me, part)], gates.at[mine_of, :])
    own_up = keep_local(up.at[:, at(me, part)], ups.at[mine_of, :])

    def pass_on(owner, i):
        return go(piece(owner, i), piece(owner, i), sibling)

    def zblock(j, b):
        if j == 0:
            return downs.at[at(b, block), :]
        return pair_w.at[at(b * 2 + (j - 1), block // 2), :]

    def nearest(k):
        a = jnp.where(edge, k, (1, 2, 0, 3)[k])
        return jnp.where(low, a, OUTER - 1 - a)

    def zown(j):
        b = zblock(j, outer)
        return [
            (outer < OUTER - 1, remote(b, b, zsend.at[j % 2, 0], zrecv.at[j, outer], above)),
            (outer > 0, remote(b, b, zsend.at[j % 2, 1], zrecv.at[j, outer], below)),
        ]

    def zstart(j, only):
        for way, (cond, c) in enumerate(zown(j)):

            @pl.when(cond & only)
            def _():
                if j == 2:
                    zown(0)[way][1].wait_send()
                c.start()

    def zcopy(j, k):
        b = nearest(k)
        target = level(jnp.clip(jnp.where(b > outer, outer - 1, outer + 1), 0, OUTER - 1))
        return remote(zblock(j, b), zblock(j, b), zsend.at[j % 2, 1 + k], zrecv.at[j, b], target)

    def zforward(j, k):
        c = zcopy(j, k)

        @pl.when(middle)
        def _():
            c.wait_recv()
            if j == 2:
                zcopy(0, k).wait_send()
            c.start()

    def zarrive(j, k):
        c = zcopy(j, k)

        @pl.when(edge)
        def _():
            c.wait_recv()

    tile = tokens // 2

    def d_hidden(owner):
        def step(i, carry):
            r = at(owner * 2 + i, tile)
            dh[r, :] = jnp.dot(cots[r, :], downs[...], preferred_element_type=F32)
            return carry

        lax.fori_loop(0, 2, step, 0)

    strip = tokens // 16
    first_cut = part // LANES * 2 // 3 * LANES
    cuts, everything = [(0, first_cut), (first_cut, part - first_cut)], (0, part)

    def pointwise(owner, cut):
        c, second = pl.ds(*cut), pl.ds(part + cut[0], cut[1])

        def step(i, carry):
            r = at(owner * 16 + i, strip)
            gv, uv, dv = gates[r, c].astype(F32), ups[r, c].astype(F32), dh[r, c]
            s = jax.nn.sigmoid(gv)
            gs = gv * s
            hidden[r, c] = (gs * uv).astype(BF16)
            dpair[r, c] = (dv * uv * s * (1.0 + gv * (1.0 - s))).astype(BF16)
            dpair[r, second] = (dv * gs).astype(BF16)
            return carry

        lax.fori_loop(0, 16, step, 0)

    span = depth // 4

    def outer_product(owner, cut, first=False, last=False):
        r, c = at(owner, tokens), pl.ds(*cut)
        turned[c, :] = hidden[r, c].T

        def step(i, carry):
            d = at(i, span)
            new = jnp.dot(turned[c, :], cots[r, d], preferred_element_type=F32)
            if not first:
                new = new + acc[c, d]
            acc[c, d] = new
            if last:
                share[c, d] = new.astype(BF16)
            return carry

        lax.fori_loop(0, 4, step, 0)

    lane = block // 2

    def product(p, owner, side, dst):
        r = at(owner, tokens)

        def step(i, carry):
            b = jnp.where(i == 0, nearest(2 * p), nearest(2 * p + 1))
            total = lax.dot_general(
                dpair[r, :], pair_w[at(b * 2 + side, lane), :], OVER, preferred_element_type=F32
            )
            dst[:, at(i, lane)] = total.astype(BF16)
            return carry

        lax.fori_loop(0, 2, step, 0)

    def add(dst, where, src):
        dst[where, :] = (dst[where, :].astype(F32) + src[...].astype(F32)).astype(BF16)

    slot = {}

    def give_away(p, n, owner):
        k = p * 4 + n
        product(p, owner, 1 - core, give.at[k])
        slot[k] = go(give.at[k], sib.at[k], sibling)

    def keep_own(p, n, owner):
        product(p, owner, core, mine.at[p * 4 + n])

    def join(p, n):
        k = p * 4 + n
        slot[k].wait_recv()
        add(mine.at[k], pl.ds(0, tokens), sib.at[k])

    top, bottom = pl.ds(0, half), pl.ds(half, half)
    crossing, arrivals = {}, {}

    def send_far(p):
        k = p * 4
        crossing[p, 0] = go(mine.at[k, top, :], halves.at[p, 0], xdev)
        crossing[p, 1] = go(mine.at[k, bottom, :], halves.at[p, 1], ydev)

    def send_x(p):
        arrivals[p, 0] = go(mine.at[p * 4 + 1, top, :], got.at[p, 0, top, :], xdev)

    def send_y(p):
        arrivals[p, 1] = go(mine.at[p * 4 + 2, bottom, :], got.at[p, 1, bottom, :], ydev)

    def relay(p):
        crossing[p, 1].wait_recv()
        add(mine.at[p * 4 + 1], bottom, halves.at[p, 1])
        arrivals[p, 2] = go(mine.at[p * 4 + 1, bottom, :], got.at[p, 0, bottom, :], xdev)
        crossing[p, 0].wait_recv()
        add(mine.at[p * 4 + 2], top, halves.at[p, 0])
        arrivals[p, 3] = go(mine.at[p * 4 + 2, top, :], got.at[p, 1, top, :], ydev)

    lasts = []

    def finish(p):
        for i in range(4):
            arrivals[p, i].wait_recv()
        for i in range(2):
            c = pl.ds(i * lane, lane)
            total = mine[p * 4 + 3, :, c].astype(F32) + got[p, 0, :, c].astype(F32) + got[p, 1, :, c].astype(F32)
            where = at(nearest(2 * p + i) * 2 + core, lane)
            out[:, where] = total.astype(BF16)
            lasts.append(go(out.at[:, where], out.at[:, where], sibling))

    near = jnp.where(low, 1 - outer, 5 - outer)
    cross_mid = jnp.where(low, 2, 1)
    cross_edge = jnp.where(low, 3, 0)
    edge_sends, near_sends, cross_sends = [], [], []
    for t, cut in enumerate(cuts):
        c = pl.ds(*cut)
        edge_sends.append([
            remote(share.at[c, at(cross_edge, block)], comb.at[1, c, :], rsend.at[t, 0], rrecv.at[t, 0], level(near)),
            remote(share.at[c, at(cross_mid, block)], comb.at[0, c, :], rsend.at[t, 1], rrecv.at[t, 1], level(near)),
        ])
        near_sends.append(
            remote(share.at[c, at(near, block)], reduced.at[0, c, :], rsend.at[t, 2], rrecv.at[t, 2], level(near))
        )
        cross_sends.append([
            remote(joined.at[1, c, :], reduced.at[1, c, :], rsend.at[t, 0], rrecv.at[t, 3], level(cross_edge)),
            remote(joined.at[0, c, :], reduced.at[1, c, :], rsend.at[t, 1], rrecv.at[t, 3], level(cross_mid)),
        ])

    def reduce_start(t):
        @pl.when(edge)
        def _():
            for c in edge_sends[t]:
                c.start()

        near_sends[t].start()

    def reduce_join(t):
        c = pl.ds(*cuts[t])

        @pl.when(middle)
        def _():
            for i, dest in ((1, cross_edge), (0, cross_mid)):
                edge_sends[t][1 - i].wait_recv()
                joined[i, c, :] = (share[c, at(dest, block)].astype(F32) + comb[i, c, :].astype(F32)).astype(BF16)
                cross_sends[t][1 - i].start()

    gd_sends = {}

    def reduce_finish():
        for t in range(2):
            near_sends[t].wait_recv()
            cross_sends[t][0].wait_recv()
        total = acc[:, at(outer, block)] + reduced[0].astype(F32) + reduced[1].astype(F32)
        final[...] = total.astype(BF16)
        for i in (2, 0, 1):
            q, d = others[i]
            gd_sends[i] = go(final.at[:, at(q, rows)], swapped.at[i], d)
        gd[:, at(me, part)] = final[:, at(me, rows)].astype(F32).T

    yes = outer >= 0
    swaps[2, 2].wait_recv()
    y1 = go(cot.at[row_half, cols[1]], piece(me, 1), ydev)
    y0 = go(cot.at[row_half, cols[0]], piece(me, 0), ydev)
    own_down.wait()
    for c in swap_down:
        c.wait_recv()
    zstart(0, yes)
    for c in own_pair:
        c.wait()
    for c in swap_pair[:-1]:
        c.wait_recv()
    for k in (1, 2):
        zforward(0, k)
        zarrive(0, k)
    for j in (1, 2):
        zstart(j, edge)
    zforward(0, 3)
    for j in (1, 2):
        zstart(j, middle)
    retire(*swap_down, *swap_pair)
    passes = {}
    x0.wait_recv()
    fy = go(piece(xn, 0), piece(xn, 0), ydev)
    passes["x", 0] = pass_on(xn, 0)
    y1.wait_recv()
    fx = go(piece(yn, 1), piece(yn, 1), xdev)
    passes["y", 1] = pass_on(yn, 1)
    arrive = {}
    saved = ((gate, gates), (up, ups))

    def give_saved(name, owner, device, cut, r, arrays):
        for a, b in arrays:
            src = a.at[r, pl.ds(pl.multiple_of(owner * part + cut[0], LANES), cut[1])]
            dst = b.at[pl.ds(pl.multiple_of(me * tokens + r.start, r.size), r.size), pl.ds(*cut)]
            arrive.setdefault((name, cut), []).append(go(src, dst, device))

    whole, late = pl.ds(0, tokens), tokens // 4
    give_saved("f", far, fdev, everything, whole, saved[:1])
    for r in (pl.ds(0, tokens // 2), pl.ds(tokens // 2, late), pl.ds(tokens - late, late)):
        give_saved("f", far, fdev, everything, r, saved[1:])
    for cut in cuts:
        give_saved("x", xn, xdev, cut, whole, saved)
    own_cot.wait()
    own_gate.wait()
    own_up.wait()
    zarrive(0, 3)
    d_hidden(me)
    pointwise(me, everything)
    outer_product(me, everything, first=True)
    x1.wait_recv()
    passes["x", 1] = pass_on(xn, 1)
    y0.wait_recv()
    passes["y", 0] = pass_on(yn, 0)
    for j in (1, 2):
        for k in (1, 2):
            zforward(j, k)
    retire(x0, y1, x1, y0)
    fy.wait_recv()
    passes["f", 0] = pass_on(far, 0)
    fx.wait_recv()
    passes["f", 1] = pass_on(far, 1)
    zforward(1, 3)
    for name, owner in (("x", xn), ("y", yn), ("f", far)):
        for i in range(2):
            passes[name, i].wait_recv()
        d_hidden(owner)
        if name == "y":
            zforward(2, 3)

    for c in arrive["f", everything][:-1]:
        c.wait_recv()
    for cut in cuts:
        give_saved("y", yn, ydev, cut, whole, saved)
    arrive["f", everything][-1].wait_recv()
    retire(fy, fx, *passes.values())
    pointwise(far, everything)
    for j in (1, 2):
        zarrive(j, 1)
    give_away(0, 0, far)
    keep_own(0, 0, far)
    give_away(0, 3, me)
    join(0, 0)
    send_far(0)
    outer_product(far, everything)
    keep_own(0, 3, me)
    join(0, 3)
    for name, owner in (("x", xn), ("y", yn)):
        for c in arrive[name, cuts[0]]:
            c.wait_recv()
        pointwise(owner, cuts[0])
        outer_product(owner, cuts[0], last=name == "y")
    reduce_start(0)
    for c in arrive["x", cuts[1]]:
        c.wait_recv()
    pointwise(xn, cuts[1])
    give_away(0, 1, xn)
    keep_own(0, 1, xn)
    for c in arrive["y", cuts[1]]:
        c.wait_recv()
    pointwise(yn, cuts[1])
    give_away(0, 2, yn)
    join(0, 1)
    send_x(0)
    keep_own(0, 2, yn)
    join(0, 2)
    send_y(0)
    outer_product(xn, cuts[1])
    relay(0)
    outer_product(yn, cuts[1], last=True)
    reduce_start(1)
    retire(*[c for cs in arrive.values() for c in cs], *slot.values(), crossing[0, 0], crossing[0, 1])
    for k in (2, 3):
        for j in (1, 2):
            zarrive(j, k)
    give_away(1, 0, far)
    keep_own(1, 0, far)
    give_away(1, 1, xn)
    join(1, 0)
    send_far(1)
    reduce_join(0)
    keep_own(1, 1, xn)
    give_away(1, 2, yn)
    join(1, 1)
    send_x(1)
    keep_own(1, 2, yn)
    give_away(1, 3, me)
    join(1, 2)
    send_y(1)
    keep_own(1, 3, me)
    join(1, 3)
    reduce_join(1)
    finish(0)
    relay(1)
    reduce_finish()
    finish(1)
    for i, (q, _) in enumerate(others):
        gd_sends[i].wait_recv()
        gd[:, at(q, part)] = swapped[i].astype(F32).T
    for c in lasts:
        c.wait_recv()
    retire(*[c for c, _ in started.values()])
    for j in (1, 2):
        for cond, c in zown(j):

            @pl.when(cond)
            def _():
                c.wait_send()

    @pl.when(middle)
    def _():
        for j in (1, 2):
            for k in (1, 2, 3):
                zcopy(j, k).wait_send()
        for c in cross_sends[0] + cross_sends[1]:
            c.wait_send()

    @pl.when(edge)
    def _():
        for c in edge_sends[0] + edge_sends[1]:
            c.wait_send()

    for c in near_sends:
        c.wait_send()


def flush_kernel(a, b, out_a, out_b, sems):
    copies = []
    for src, dst, pieces in ((a, out_a, 1), (b, out_b, 1)):
        rows = src.shape[0] // pieces
        for i in range(pieces):
            r = pl.ds(i * rows, rows)
            copies.append(pltpu.make_async_copy(src.at[r, :], dst.at[r, :], sems.at[len(copies)]))
    for c in copies:
        c.start()
    for c in copies:
        c.wait()


def layer(gate_pre, up_pre, cotangent, gate_weight, up_weight, down_weight):
    tokens, width = gate_pre.shape
    rows, depth = gate_weight.shape[0], cotangent.shape[1]
    g = GROUP
    part, block, everyone = width // g, rows * g, tokens * g
    lane, half = block // 2, tokens // 2
    sems, vmem = pltpu.SemaphoreType.DMA, pltpu.VMEM
    struct = jax.ShapeDtypeStruct
    hbm = pl.BlockSpec(memory_space=pl.ANY)
    whole = pl.BlockSpec(memory_space=pltpu.VMEM)
    made = pl.pallas_call(
        layer_kernel,
        out_shape=[vmem((tokens, depth), BF16), vmem((rows, width), F32)],
        in_specs=[hbm] * 6,
        out_specs=[whole] * 2,
        scratch_shapes=[
            vmem((everyone, depth), BF16),
            vmem((depth, part), BF16),
            vmem((depth, 2 * part), BF16),
            vmem((everyone, part), BF16),
            vmem((everyone, part), BF16),
            vmem((everyone, part), F32),
            vmem((everyone, part), BF16),
            vmem((everyone, 2 * part), BF16),
            vmem((part, depth), F32),
            vmem((part, depth), BF16),
            vmem((PARTS * 4, tokens, 2 * lane), BF16),
            vmem((PARTS * 4, tokens, 2 * lane), BF16),
            vmem((PARTS * 4, tokens, 2 * lane), BF16),
            vmem((PARTS, 2, tokens, 2 * lane), BF16),
            vmem((PARTS, 2, half, 2 * lane), BF16),
            vmem((2, part, block), BF16),
            vmem((2, part, block), BF16),
            vmem((2, part, block), BF16),
            vmem((part, block), BF16),
            vmem((3, part, rows), BF16),
            vmem((part, tokens), BF16),
            vmem((rows, width), BF16),
            sems((SEND_SLOTS,)), sems((RECV_SLOTS,)), sems((2, 5)), sems((3, OUTER)), sems((2, 3)), sems((2, 4)), sems((7,)),
            pltpu.SemaphoreType.REGULAR,
        ],
        compiler_params=pltpu.CompilerParams(
            collective_id=0, has_side_effects=True, vmem_limit_bytes=VMEM_LIMIT
        ),
    )(cotangent, gate_pre, up_pre, gate_weight, up_weight, down_weight)
    return pl.pallas_call(
        flush_kernel,
        out_shape=[struct((tokens, depth), BF16), struct((rows, width), F32)],
        in_specs=[whole] * 2,
        out_specs=[hbm] * 2,
        scratch_shapes=[sems((2,))],
        compiler_params=pltpu.CompilerParams(vmem_limit_bytes=4 * 1024 * 1024),
    )(*[pltpu.with_memory_space_constraint(m, pltpu.VMEM) for m in made])


def plain(gate_pre, up_pre, cotangent, gate_weight, up_weight, down_weight):
    gate = gate_pre.astype(F32)
    upper = up_pre.astype(F32)
    sigma = jax.nn.sigmoid(gate)
    hidden = (gate * sigma * upper).astype(BF16)
    share = lax.dot_general(cotangent, hidden, DOWN, preferred_element_type=F32)
    grad_down = lax.psum_scatter(share, "fs", scatter_dimension=0, tiled=True)
    d_hidden = jnp.dot(cotangent, lax.all_gather(down_weight, "fs", axis=0, tiled=True), preferred_element_type=F32)
    d_gate = (d_hidden * upper * sigma * (1.0 + gate * (1.0 - sigma))).astype(BF16)
    d_up = (d_hidden * gate * sigma).astype(BF16)
    gate_w, up_w = lax.all_gather((gate_weight, up_weight), "fs", axis=0, tiled=True)
    partial_sum = lax.dot_general(d_gate, gate_w, OVER, preferred_element_type=F32)
    partial_sum = partial_sum + lax.dot_general(d_up, up_w, OVER, preferred_element_type=F32)
    grad_input = lax.psum(partial_sum.astype(BF16), "tp").astype(F32).astype(BF16)
    return grad_input, grad_down


def solution(mesh):
    n_fs, n_tp = mesh.shape["fs"], mesh.shape["tp"]

    def local(*args):
        tokens, width = args[0].shape
        rows, depth = args[3].shape[0], args[2].shape[1]
        fits = n_tp == 2 and n_fs == GROUP * OUTER and width % (GROUP * LANES) == 0 and width >= 2 * GROUP * LANES
        fits = fits and rows % LANES == 0 and tokens % 512 == 0 and depth == rows * n_fs
        return layer(*args) if fits else plain(*args)

    both, rows = P("fs", "tp"), P("fs", None)
    return jax.shard_map(
        local, mesh=mesh, in_specs=(both, both, rows, both, both, both), out_specs=(rows, both), check_vma=False
    )
```
